256 devices in a mesh: ep: 64 (over z, x, core), tp: 4 (over y).
Axes of the slice: x: 4, y: 4, z: 8, core: 2. Of those that a mesh axis runs over, the one named last changes fastest.
Arguments:
- conv_value: bfloat16 [65536, 1024], P('ep', 'tp'), may hold values from -600 to 600
- conv_gate: bfloat16 [65536, 1024], P('ep', 'tp'), may hold values from -8 to 8
- depth_weight: float32 [31, 1024], replicated, may hold values from -1 to 1
- norm_gain: float32 [1024], replicated, may hold values from 0.1 to 1.9
- norm_shift: float32 [1024], replicated, may hold values from -3 to 3
- conv_out_weight: bfloat16 [1024, 2048], P('tp'), may hold values from -0.1875 to 0.1875
- moe_input: bfloat16 [98304, 2048], P(('ep', 'tp')), may hold values from -6 to 6
- moe_gain: float32 [2048], replicated, may hold values from 0.1 to 1.9
- route_experts: int32 [98304, 2], P(('ep', 'tp')), may hold values from 0 to 63, as said below
- route_scores: float32 [98304, 2], P(('ep', 'tp')), may hold values from -8 to 8
- expert_gate: bfloat16 [64, 2048, 512], P('ep'), may hold values from -0.125 to 0.125
- expert_up: bfloat16 [64, 2048, 512], P('ep'), may hold values from -0.125 to 0.125
- expert_down: bfloat16 [64, 512, 2048], P('ep'), may hold values from -1 to 1
Outputs:
- conv_out: bfloat16 [65536, 2048], P(('ep', 'tp'))
- moe_out: bfloat16 [98304, 2048], P(('ep', 'tp'))
The draws below stay inside these ranges and needn't reach their ends.
Inputs may be any that keep to these rules, and one draw needn't show every extreme that they name: `route_experts`: each row names two different experts that lie in one group of 16 consecutive experts.
All inputs are finite; a program needn't handle non-finite values.
Results may differ from the reference program's by a relative error of at most 0.009.
Values may be sent and summed in bfloat16 or wider, within the bound.
No kernel may reach another device: no remote copies, remote signals or barrier semaphores. Data moves between devices by JAX's collectives and lax.ppermute only.
A program may use at most 128 MiB of HBM per device.

```python
import jax
import jax.numpy as jnp
from jax import lax

D = 2048
CONV = 1024
FF = 512
KERNEL = 31
GROUPS = 4
TOP = 2
TOK_B = 384
EXPERTS = 64
GROUP_EXP = 16
CAP = 18
TOKENS_A = 65536
TOKENS_B = 98304
N_EP = 64
N_TP = 4


def draw_conv_value(key, part):
    keys = jax.random.split(jax.random.fold_in(key, 31), 2)
    column_scale = 10.0 ** (jnp.arange(CONV, dtype=jnp.float32) / CONV)
    base = jnp.clip(jax.random.normal(keys[0], (TOKENS_A, CONV), jnp.float32), -4.0, 4.0)
    row_scale = 10.0 ** jax.random.uniform(keys[1], (TOKENS_A, 1), jnp.float32)
    return (base * row_scale * column_scale[None, :]).astype(jnp.bfloat16)


def group_order(key):
    return jax.random.permutation(key, GROUP_EXP)


def draw_route_experts(key, part):
    keys = jax.random.split(jax.random.fold_in(key, 17), 7)
    order_groups = jax.random.permutation(keys[0], GROUPS)
    group_pick = jnp.minimum(jax.random.randint(keys[1], (TOKENS_B,), 0, GROUPS), jax.random.randint(keys[2], (TOKENS_B,), 0, GROUPS))
    group_id = order_groups[group_pick]
    orders = jax.vmap(group_order)(jax.random.split(keys[3], GROUPS))
    first_pick = jnp.minimum(jax.random.randint(keys[4], (TOKENS_B,), 0, GROUP_EXP), jax.random.randint(keys[5], (TOKENS_B,), 0, GROUP_EXP))
    second_pick = (first_pick + 1 + jax.random.randint(keys[6], (TOKENS_B,), 0, GROUP_EXP - 1)) % GROUP_EXP
    first = group_id * GROUP_EXP + orders[group_id, first_pick]
    second = group_id * GROUP_EXP + orders[group_id, second_pick]
    return jnp.stack([first, second], axis=1).astype(jnp.int32)


def shard_levels(rng, dims, shards, smallest, top_value):
    def one(position, shards_of):
        steps = jax.random.uniform(jax.random.fold_in(jax.random.fold_in(rng, 6), position), (shards_of,), jnp.float32, smallest / len(shards), top_value / len(shards))
        return jnp.repeat(jnp.exp(steps), dims[position] // shards_of).reshape((-1,) + (1,) * (len(dims) - position - 1))

    gain = one(*shards[0])
    for cut in shards[1:]:
        gain = gain * one(*cut)
    return gain


def normal_values(key, dims, deviation, reach, cuts=(), kind=jnp.bfloat16):
    result = jax.random.normal(key, dims, jnp.float32) * deviation
    if len(cuts) > 0:
        result = shard_levels(key, dims, cuts, -0.22, 0.18) * result
    return jnp.clip(result, min=-reach, max=reach).astype(kind)


def setup_inputs(seed: int = 0) -> dict:
    arg_keys = jax.random.split(jax.random.key(seed), 14)
    conv_value = draw_conv_value(jax.random.fold_in(arg_keys[13], 71), 0)
    conv_gate = normal_values(arg_keys[1], (TOKENS_A, CONV), 1.5, 8.0, ((0, 64), (1, 4)))
    depth_weight = normal_values(arg_keys[2], (KERNEL, CONV), KERNEL ** -0.5, 1.0, (), jnp.float32)
    norm_gain = jnp.clip(1.0 + 0.18 * jax.random.normal(arg_keys[3], (CONV,), jnp.float32), 0.1, 1.9)
    norm_shift = normal_values(arg_keys[4], (CONV,), 0.5, 3.0, (), jnp.float32)
    conv_out_weight = normal_values(arg_keys[5], (CONV, D), CONV ** -0.5, 0.1875, ((0, 4),))
    moe_input = normal_values(arg_keys[6], (TOKENS_B, D), 1.0, 6.0, ((0, 256),))
    moe_gain = jnp.clip(1.0 + 0.18 * jax.random.normal(arg_keys[7], (D,), jnp.float32), 0.1, 1.9)
    route_experts = draw_route_experts(jax.random.fold_in(arg_keys[13], 71), 0)
    route_scores = normal_values(arg_keys[9], (TOKENS_B, TOP), 1.5, 8.0, ((0, 256),), jnp.float32)
    expert_gate = normal_values(arg_keys[10], (EXPERTS, D, FF), D ** -0.5, 0.125, ((0, 64),))
    expert_up = normal_values(arg_keys[11], (EXPERTS, D, FF), D ** -0.5, 0.125, ((0, 64),))
    expert_down = normal_values(arg_keys[12], (EXPERTS, FF, D), (FF // 16) ** -0.5, 1.0, ((0, 64),))
    return dict(conv_value=conv_value, conv_gate=conv_gate, depth_weight=depth_weight, norm_gain=norm_gain, norm_shift=norm_shift, conv_out_weight=conv_out_weight, moe_input=moe_input, moe_gain=moe_gain, route_experts=route_experts, route_scores=route_scores, expert_gate=expert_gate, expert_up=expert_up, expert_down=expert_down)


def conv_part(conv_value, conv_gate, depth_weight, norm_gain, norm_shift, conv_out_weight):
    gated = (conv_value.astype(jnp.float32) * jax.nn.sigmoid(conv_gate.astype(jnp.float32))).astype(jnp.bfloat16)
    padded = jnp.concatenate([jnp.zeros((KERNEL - 1, CONV), jnp.bfloat16), gated], 0).astype(jnp.float32)
    filtered = jnp.zeros((TOKENS_A, CONV), jnp.float32)
    for offset in range(KERNEL):
        filtered = filtered + depth_weight[offset] * padded[offset:offset + TOKENS_A]
    center = lax.optimization_barrier(jnp.mean(filtered, axis=-1, keepdims=True))
    spread = lax.optimization_barrier(jnp.mean(filtered * filtered, axis=-1, keepdims=True)) - center * center
    normed = (filtered - center) * lax.rsqrt(spread + 1e-05) * norm_gain + norm_shift
    activated = jax.nn.silu(normed).astype(jnp.bfloat16)
    block_width = CONV // N_TP
    summed = jnp.zeros((TOKENS_A, D), jnp.float32)
    for column_block in range(N_TP):
        low = column_block * block_width
        partial_value = jnp.dot(activated[:, low:low + block_width], conv_out_weight[low:low + block_width], preferred_element_type=jnp.float32).astype(jnp.bfloat16)
        summed = summed + partial_value.astype(jnp.float32)
    return summed.astype(jnp.bfloat16)

def moe_part(moe_input, moe_gain, route_experts, route_scores, expert_gate, expert_up, expert_down):
    widened = moe_input.astype(jnp.float32)
    normal_in = (widened * lax.rsqrt(lax.optimization_barrier(jnp.mean(widened * widened, axis=-1, keepdims=True)) + 1e-06) * moe_gain).astype(jnp.bfloat16)
    sources = N_EP * N_TP
    chosen = route_experts.reshape(sources, TOK_B * TOP)
    onehot = (chosen[:, :, None] == jnp.arange(EXPERTS, dtype=jnp.int32)[None, None, :]).astype(jnp.int32)
    slot_rank = lax.optimization_barrier(jnp.sum(jnp.cumsum(onehot, axis=1) * onehot, axis=-1)) - 1
    within_cap = slot_rank < CAP
    source_ids = jnp.arange(sources, dtype=jnp.int32)[:, None]
    token_index = source_ids * TOK_B + jnp.arange(TOK_B * TOP, dtype=jnp.int32)[None, :] // TOP
    per_expert = sources * CAP
    slot_index = jnp.where(within_cap, chosen * per_expert + source_ids * CAP + slot_rank, EXPERTS * per_expert).astype(jnp.int32)
    slot_token = jnp.full((EXPERTS * per_expert,), TOKENS_B, jnp.int32).at[slot_index.reshape(-1)].set(token_index.reshape(-1), mode='drop')
    group_gate = jax.nn.sigmoid(route_scores[:, 0])
    weights = jnp.stack([group_gate * jax.nn.sigmoid(route_scores[:, 1]), group_gate * jax.nn.sigmoid(-route_scores[:, 1])], axis=-1)
    slot_weight = jnp.zeros((EXPERTS * per_expert,), jnp.float32).at[slot_index.reshape(-1)].set(weights.reshape(-1), mode='drop')
    padded_in = jnp.concatenate([normal_in, jnp.zeros((1, D), jnp.bfloat16)], 0)

    def apply_expert(summed, inputs):
        gate_matrix, up_matrix, down_matrix, tokens_here, weight_here = inputs
        picked_rows = padded_in[tokens_here]
        gate_act = jnp.dot(picked_rows, gate_matrix, preferred_element_type=jnp.float32)
        up_act = jnp.dot(picked_rows, up_matrix, preferred_element_type=jnp.float32)
        inner = (jax.nn.silu(gate_act) * up_act).astype(jnp.bfloat16)
        expert_rows = jnp.dot(inner, down_matrix, preferred_element_type=jnp.float32).astype(jnp.bfloat16)
        summed = summed.at[tokens_here].add(weight_here[:, None] * expert_rows.astype(jnp.float32), mode='drop')
        return (summed, None)
    summed, _ = lax.scan(apply_expert, jnp.zeros((TOKENS_B, D), jnp.float32), (expert_gate, expert_up, expert_down, slot_token.reshape(EXPERTS, per_expert), slot_weight.reshape(EXPERTS, per_expert)))
    return summed.astype(jnp.bfloat16)

def reference(conv_value, conv_gate, depth_weight, norm_gain, norm_shift, conv_out_weight, moe_input, moe_gain, route_experts, route_scores, expert_gate, expert_up, expert_down):
    conv_out = conv_part(conv_value, conv_gate, depth_weight, norm_gain, norm_shift, conv_out_weight)
    moe_out = moe_part(moe_input, moe_gain, route_experts, route_scores, expert_gate, expert_up, expert_down)
    return (conv_out, moe_out)
```

```python
import jax
import jax.numpy as jnp
from jax import lax
from jax.experimental import pallas as pl
from jax.experimental.pallas import tpu as pltpu
from jax.sharding import PartitionSpec as P

CONV = 1024
TOP = 2
MAIN = 16
EXTRA = 2
PIECE = 256
PIECES = 8
GROUP = 16


def passed_along(x, axis, by):
    peers = lax.axis_size(axis)
    pairs = [(i, i + by) for i in range(peers) if 0 <= i + by < peers]
    return lax.ppermute(x, axis, pairs)


def iota(shape, dimension):
    return lax.broadcasted_iota(jnp.int32, shape, dimension)


def fold_matrix():
    i = iota((PIECE, PIECE), 0)
    c = iota((PIECE, PIECE), 1)
    return (c == (i % PIECES) * (2 * GROUP) + i // PIECES).astype(jnp.bfloat16)


def unfold_matrix():
    i = iota((PIECE, PIECE), 1)
    c = iota((PIECE, PIECE), 0)
    return (c == (i % PIECES) * (2 * GROUP) + i // PIECES).astype(jnp.bfloat16)


def dot(a, b):
    return jnp.dot(a, b, preferred_element_type=jnp.float32)


def folded(rows):
    stacked = jnp.concatenate([rows[:, PIECE * k : PIECE * (k + 1)] for k in range(PIECES)], 0)
    return dot(fold_matrix(), stacked).astype(jnp.bfloat16)


def unfolded(block):
    stacked = dot(unfold_matrix(), block).astype(jnp.bfloat16)
    n = 2 * GROUP
    return jnp.concatenate([stacked[n * k : n * (k + 1)] for k in range(PIECES)], 1)


def send_kernel(route_ref, x_ref, gain_ref, send_ref, xn_ref, ids_ref):
    tokens, width = x_ref.shape
    experts = send_ref.shape[0]
    chunk = 32

    def norm(i, carry):
        rows = pl.ds(pl.multiple_of(i * chunk, chunk), chunk)
        x = x_ref[rows, :].astype(jnp.float32)
        scale = lax.rsqrt(jnp.mean(x * x, axis=-1, keepdims=True) + 1e-06)
        xn_ref[rows, :] = (x * scale * gain_ref[...]).astype(jnp.bfloat16)
        return carry

    lax.fori_loop(0, tokens // chunk, norm, 0)

    expert = iota((experts, tokens), 0)
    first, second = route_ref[0:1, :], route_ref[1:2, :]
    is_first, is_second = expert == first, expert == second
    hits = (is_first | is_second).astype(jnp.bfloat16)
    earlier = (iota((tokens, tokens), 0) < iota((tokens, tokens), 1)).astype(jnp.bfloat16)
    counts = dot(hits, earlier)
    for row, (mask, named) in enumerate(((is_first, first), (is_second, second))):
        rank = jnp.sum(jnp.where(mask, counts, 0.0), axis=0, keepdims=True).astype(jnp.int32)
        main = jnp.where(rank < MAIN, named * MAIN + rank, -1)
        extra = jnp.where((rank >= MAIN) & (rank < MAIN + EXTRA), named * EXTRA + rank - MAIN, -1)
        ids_ref[row : row + 1, :] = main
        ids_ref[row + 2 : row + 3, :] = extra

    def group(g, carry):
        row = iota((GROUP * MAIN, tokens), 0) + g * (GROUP * MAIN)
        pick = ((row == ids_ref[0:1, :]) | (row == ids_ref[1:2, :])).astype(jnp.bfloat16)
        low = iota((GROUP * EXTRA, tokens), 0) + g * (GROUP * EXTRA)
        more = ((low == ids_ref[2:3, :]) | (low == ids_ref[3:4, :])).astype(jnp.bfloat16)
        here = pl.ds(g * GROUP, GROUP)
        send_ref[here, :, 0:width] = (
            dot(pick, xn_ref[...]).astype(jnp.bfloat16).reshape(GROUP, MAIN, width)
        )
        rest = dot(more, xn_ref[...]).astype(jnp.bfloat16)
        send_ref[here, :, width:] = folded(rest).reshape(GROUP, MAIN, PIECE)
        return carry

    lax.fori_loop(0, experts // GROUP, group, 0)


def expert_kernel(in_ref, gate_ref, up_ref, down_ref, out_ref):
    width = gate_ref.shape[0]
    sources = in_ref.shape[0]
    both = 2

    def block(b, carry):
        parts = []
        for j in range(both):
            here = pl.ds((b * both + j) * GROUP, GROUP)
            parts.append(in_ref[here, :, 0:width].reshape(GROUP * MAIN, width))
        for j in range(both):
            here = pl.ds((b * both + j) * GROUP, GROUP)
            parts.append(unfolded(in_ref[here, :, width:].reshape(PIECE, PIECE)))
        rows = jnp.concatenate(parts, 0)
        gate = dot(rows, gate_ref[...])
        up = dot(rows, up_ref[...])
        inner = (gate / (1.0 + jnp.exp(-gate)) * up).astype(jnp.bfloat16)
        result = dot(inner, down_ref[...]).astype(jnp.bfloat16)
        for j in range(both):
            here = pl.ds((b * both + j) * GROUP, GROUP)
            top = j * GROUP * MAIN
            out_ref[here, :, 0:width] = result[top : top + GROUP * MAIN].reshape(GROUP, MAIN, width)
            low = both * GROUP * MAIN + j * GROUP * EXTRA
            out_ref[here, :, width:] = folded(result[low : low + GROUP * EXTRA]).reshape(
                GROUP, MAIN, PIECE
            )
        return carry

    lax.fori_loop(0, sources // (GROUP * both), block, 0)


def weight_kernel(route_ref, score_ref, main_ref, extra_ref):
    tokens = route_ref.shape[0]
    experts = main_ref.shape[1] // MAIN
    expert = iota((tokens, experts), 1)
    first, second = route_ref[:, 0:1], route_ref[:, 1:2]
    is_first, is_second = expert == first, expert == second
    hits = (is_first | is_second).astype(jnp.bfloat16)
    earlier = (iota((tokens, tokens), 0) > iota((tokens, tokens), 1)).astype(jnp.bfloat16)
    counts = dot(earlier, hits)
    group = jax.nn.sigmoid(score_ref[:, 0:1])
    pair = score_ref[:, 1:2]
    weights = (group * jax.nn.sigmoid(pair), group * jax.nn.sigmoid(-pair))
    places = []
    for mask, named in ((is_first, first), (is_second, second)):
        rank = jnp.sum(jnp.where(mask, counts, 0.0), axis=1, keepdims=True).astype(jnp.int32)
        places.append(
            (
                jnp.where(rank < MAIN, named * MAIN + rank, -1),
                jnp.where((rank >= MAIN) & (rank < MAIN + EXTRA), named * EXTRA + rank - MAIN, -1),
            )
        )
    for ref, which in ((main_ref, 0), (extra_ref, 1)):
        n = ref.shape[1]
        step = min(n, 256)
        for low in range(0, n, step):
            column = iota((tokens, step), 1) + low
            value = jnp.where(column == places[0][which], weights[0], 0.0)
            value = jnp.where(column == places[1][which], weights[1], value)
            high = value.astype(jnp.bfloat16)
            ref[0:tokens, low : low + step] = high
            ref[tokens:, low : low + step] = (value - high.astype(jnp.float32)).astype(jnp.bfloat16)


def combine_kernel(back_ref, main_ref, extra_ref, out_ref, rest_ref):
    experts, _, wide = back_ref.shape
    width = wide - PIECE
    tokens = out_ref.shape[0]
    for g in range(experts // GROUP):
        block = back_ref[g * GROUP : (g + 1) * GROUP, :, width:].reshape(PIECE, PIECE)
        rest_ref[g * 2 * GROUP : (g + 1) * 2 * GROUP, :] = unfolded(block)
    step = 256

    def columns(i, carry):
        here = pl.ds(pl.multiple_of(i * step, step), step)
        rows = back_ref[:, :, here].reshape(experts * MAIN, step)
        total = dot(main_ref[...], rows) + dot(extra_ref[...], rest_ref[:, here])
        out_ref[:, here] = (total[:tokens] + total[tokens:]).astype(jnp.bfloat16)
        return carry

    lax.fori_loop(0, width // step, columns, 0)


VMEM = pl.BlockSpec(memory_space=pltpu.VMEM)


def call(kernel, name, outs, scratch, limit, flops, nbytes, *args):
    return pl.pallas_call(
        kernel,
        name=name,
        out_shape=outs,
        in_specs=[VMEM] * len(args),
        out_specs=jax.tree.map(lambda _: VMEM, outs),
        scratch_shapes=scratch,
        compiler_params=pltpu.CompilerParams(vmem_limit_bytes=limit << 20),
        cost_estimate=pl.CostEstimate(flops=flops, bytes_accessed=nbytes, transcendentals=0),
    )(*args)


def conv_half(conv_value, conv_gate, depth_weight, norm_gain, norm_shift, conv_out_weight):
    channels = conv_value.shape[1]
    length = conv_value.shape[0]
    first_col = lax.axis_index("tp") * channels
    taps = lax.dynamic_slice_in_dim(depth_weight, first_col, channels, 1)
    gains = lax.dynamic_slice_in_dim(norm_gain, first_col, channels, 0)
    shifts = lax.dynamic_slice_in_dim(norm_shift, first_col, channels, 0)
    gated = (conv_value.astype(jnp.float32) * jax.nn.sigmoid(conv_gate.astype(jnp.float32))).astype(
        jnp.bfloat16
    )
    reach = taps.shape[0] - 1
    earlier = passed_along(gated[length - reach :], "ep", 1)
    padded = jnp.concatenate([earlier, gated], 0).astype(jnp.float32)
    filtered = taps[0] * padded[0:length]
    for offset in range(1, reach + 1):
        filtered = filtered + taps[offset] * padded[offset : offset + length]
    sums, squares = lax.psum(
        (jnp.sum(filtered, axis=1), jnp.sum(filtered * filtered, axis=1)), "tp"
    )
    center = (sums / CONV)[:, None]
    spread = (squares / CONV)[:, None] - center * center
    normed = (filtered - center) * lax.rsqrt(spread + 1e-05) * gains + shifts
    activated = jax.nn.silu(normed).astype(jnp.bfloat16)
    partial = jnp.dot(activated, conv_out_weight, preferred_element_type=jnp.float32).astype(
        jnp.bfloat16
    )
    peers = lax.axis_size("tp")
    me = lax.axis_index("tp")
    rows = length // peers
    total = lax.dynamic_slice_in_dim(partial, me * rows, rows, 0).astype(jnp.float32)
    for by in range(1, peers):
        theirs = lax.dynamic_slice_in_dim(partial, ((me + by) % peers) * rows, rows, 0)
        came = lax.ppermute(theirs, "tp", [(i, (i + by) % peers) for i in range(peers)])
        total = total + came.astype(jnp.float32)
    return total.astype(jnp.bfloat16)


def moe_half(moe_input, moe_gain, route_experts, route_scores, expert_gate, expert_up, expert_down):
    tokens, width = moe_input.shape
    experts = lax.axis_size("ep")
    hidden = expert_gate.shape[2]
    slots = experts * (MAIN + EXTRA)
    wide = jax.ShapeDtypeStruct((experts, MAIN, width + PIECE), jnp.bfloat16)
    send = call(
        send_kernel,
        "send",
        wide,
        [pltpu.VMEM((tokens, width), jnp.bfloat16), pltpu.VMEM((8, tokens), jnp.int32)],
        24,
        2 * slots * tokens * width,
        slots * width * 4,
        route_experts.T,
        moe_input,
        moe_gain[None, :],
    )
    arrived = lax.all_to_all(send, "ep", split_axis=0, concat_axis=0, tiled=True)
    main, extra = call(
        weight_kernel,
        "weights",
        (
            jax.ShapeDtypeStruct((2 * tokens, experts * MAIN), jnp.bfloat16),
            jax.ShapeDtypeStruct((2 * tokens, experts * EXTRA), jnp.bfloat16),
        ),
        [],
        16,
        2 * tokens * tokens * experts,
        4 * tokens * slots,
        route_experts,
        route_scores,
    )
    result = call(
        expert_kernel,
        "expert",
        wide,
        [],
        24,
        6 * slots * width * hidden,
        slots * width * 4,
        arrived,
        expert_gate[0],
        expert_up[0],
        expert_down[0],
    )
    returned = lax.all_to_all(result, "ep", split_axis=0, concat_axis=0, tiled=True)
    return call(
        combine_kernel,
        "combine",
        jax.ShapeDtypeStruct((tokens, width), jnp.bfloat16),
        [pltpu.VMEM((experts * EXTRA, width), jnp.bfloat16)],
        16,
        4 * slots * tokens * width,
        slots * width * 2,
        returned,
        main,
        extra,
    )


def on_device(
    conv_value,
    conv_gate,
    depth_weight,
    norm_gain,
    norm_shift,
    conv_out_weight,
    moe_input,
    moe_gain,
    route_experts,
    route_scores,
    expert_gate,
    expert_up,
    expert_down,
):
    conv_out = conv_half(
        conv_value, conv_gate, depth_weight, norm_gain, norm_shift, conv_out_weight
    )
    moe_out = moe_half(
        moe_input, moe_gain, route_experts, route_scores, expert_gate, expert_up, expert_down
    )
    return (conv_out, moe_out)


def solution(mesh):
    in_specs = (
        P("ep", "tp"),
        P("ep", "tp"),
        P(),
        P(),
        P(),
        P("tp", None),
        P(("ep", "tp"), None),
        P(),
        P(("ep", "tp"), None),
        P(("ep", "tp"), None),
        P("ep", None, None),
        P("ep", None, None),
        P("ep", None, None),
    )
    out_specs = (P(("ep", "tp"), None), P(("ep", "tp"), None))
    return jax.shard_map(
        on_device, mesh=mesh, in_specs=in_specs, out_specs=out_specs, check_vma=False
    )
```

```python
import jax
import jax.numpy as jnp
from jax import lax
from jax.experimental import pallas as pl
from jax.experimental.pallas import tpu as pltpu
from jax.sharding import PartitionSpec as P


CONV = 1024
TOP = 2
MAIN = 16
EXTRA = 2
PIECE = 256
PIECES = 8
GROUP = 16


AXES = ("pair", "member", "tp")
HALO = [(i, i + 4) for i in range(252)]


def iota(shape, dimension):
    return lax.broadcasted_iota(jnp.int32, shape, dimension)


def fold_matrix():
    i = iota((PIECE, PIECE), 0)
    c = iota((PIECE, PIECE), 1)
    return (c == (i % PIECES) * (2 * GROUP) + i // PIECES).astype(jnp.bfloat16)


def unfold_matrix():
    i = iota((PIECE, PIECE), 1)
    c = iota((PIECE, PIECE), 0)
    return (c == (i % PIECES) * (2 * GROUP) + i // PIECES).astype(jnp.bfloat16)


def dot(a, b):
    return jnp.dot(a, b, preferred_element_type=jnp.float32)


def folded(rows):
    stacked = jnp.concatenate([rows[:, PIECE * k : PIECE * (k + 1)] for k in range(PIECES)], 0)
    return dot(fold_matrix(), stacked).astype(jnp.bfloat16)


def unfolded(block):
    stacked = dot(unfold_matrix(), block).astype(jnp.bfloat16)
    n = 2 * GROUP
    return jnp.concatenate([stacked[n * k : n * (k + 1)] for k in range(PIECES)], 1)


def member_of(expert, pair):
    z, column, core = expert // 8, expert % 8, expert % 2
    ahead = (z - 2 * pair) % 8
    plane = ((ahead >= 1) & (ahead <= 4)).astype(jnp.int32)
    hops = jnp.where(plane == 1, ahead - 1, (8 - ahead) % 8)
    host = column + 1 - 2 * core
    return (plane * 8 + host) * 4 + jnp.where(core == 1, hops, 3 - hops)


def weight_pairs():
    pairs = []
    for device in range(256):
        z, x, core, y = device // 32, device // 8 % 4, device // 4 % 2, device % 4
        hops = y if core == 0 else 3 - y
        source = (z + hops if z % 2 else z - hops) % 8
        pairs.append((((source * 4 + x) * 2 + 1 - core) * 4 + y, device))
    return pairs


def send_kernel(pair_ref, route_in, x_in, gain_in, send_out, route_ref, x_ref, gain_ref, xn_ref, ids_ref, send_ref, sems):
    tokens, width = x_ref.shape
    experts = send_ref.shape[0]
    chunk = 96
    chunks = tokens // chunk
    loads = [
        pltpu.make_async_copy(route_in, route_ref, sems.at[0]),
        pltpu.make_async_copy(gain_in, gain_ref, sems.at[1]),
    ]
    for i in range(chunks):
        rows = pl.ds(i * chunk, chunk)
        loads.append(pltpu.make_async_copy(x_in.at[rows], x_ref.at[rows], sems.at[2 + i]))
    for load in loads:
        load.start()
    loads[0].wait()
    pair = pair_ref[0]
    expert = iota((experts, tokens), 0)
    first, second = route_ref[0:1, :], route_ref[1:2, :]
    is_first, is_second = expert == first, expert == second
    hits = (is_first | is_second).astype(jnp.bfloat16)
    earlier = (iota((tokens, tokens), 0) < iota((tokens, tokens), 1)).astype(jnp.bfloat16)
    counts = dot(hits, earlier)
    for row, (mask, named) in enumerate(((is_first, first), (is_second, second))):
        rank = jnp.sum(jnp.where(mask, counts, 0.0), axis=0, keepdims=True).astype(jnp.int32)
        place = member_of(named, pair)
        main = jnp.where(rank < MAIN, place * MAIN + rank, -1)
        extra = jnp.where((rank >= MAIN) & (rank < MAIN + EXTRA), place * EXTRA + rank - MAIN, -1)
        ids_ref[row : row + 1, :] = main
        ids_ref[row + 2 : row + 3, :] = extra
    loads[1].wait()
    step = 32
    for i in range(chunks):
        loads[2 + i].wait()

        def norm(k, carry):
            rows = pl.ds(pl.multiple_of(i * chunk + k * step, step), step)
            x = x_ref[rows, :].astype(jnp.float32)
            scale = lax.rsqrt(jnp.mean(x * x, axis=-1, keepdims=True) + 1e-06)
            xn_ref[rows, :] = (x * scale * gain_ref[...]).astype(jnp.bfloat16)
            return carry

        lax.fori_loop(0, chunk // step, norm, 0)
    stores = []
    for g in range(experts // GROUP):
        row = iota((GROUP * MAIN, tokens), 0) + g * (GROUP * MAIN)
        pick = ((row == ids_ref[0:1, :]) | (row == ids_ref[1:2, :])).astype(jnp.bfloat16)
        low = iota((GROUP * EXTRA, tokens), 0) + g * (GROUP * EXTRA)
        more = ((low == ids_ref[2:3, :]) | (low == ids_ref[3:4, :])).astype(jnp.bfloat16)
        here = pl.ds(g * GROUP, GROUP)
        send_ref[here, :, 0:width] = (
            dot(pick, xn_ref[...]).astype(jnp.bfloat16).reshape(GROUP, MAIN, width)
        )
        rest = dot(more, xn_ref[...]).astype(jnp.bfloat16)
        send_ref[here, :, width:] = folded(rest).reshape(GROUP, MAIN, PIECE)
        stores.append(pltpu.make_async_copy(send_ref.at[here], send_out.at[here], sems.at[2 + chunks + g]))
        stores[-1].start()
    for store in stores:
        store.wait()


def hidden_kernel(in_ref, gate_ref, up_ref, out_ref):
    width = gate_ref.shape[0]
    sources = in_ref.shape[0]
    both = out_ref.shape[1] // (GROUP * (MAIN + EXTRA))

    def block(b, carry):
        parts = []
        for j in range(both):
            here = pl.ds((b * both + j) * GROUP, GROUP)
            parts.append(in_ref[here, :, 0:width].reshape(GROUP * MAIN, width))
        for j in range(both):
            here = pl.ds((b * both + j) * GROUP, GROUP)
            parts.append(unfolded(in_ref[here, :, width:].reshape(PIECE, PIECE)))
        rows = jnp.concatenate(parts, 0)
        gate = dot(rows, gate_ref[...])
        up = dot(rows, up_ref[...])
        out_ref[b] = (gate / (1.0 + jnp.exp(-gate)) * up).astype(jnp.bfloat16)
        return carry

    lax.fori_loop(0, sources // (GROUP * both), block, 0)


def down_kernel(in_ref, down_ref, out_ref):
    width = down_ref.shape[1]
    blocks, rows, _ = in_ref.shape
    both = rows // (GROUP * (MAIN + EXTRA))

    def block(b, carry):
        result = dot(in_ref[b], down_ref[...]).astype(jnp.bfloat16)
        for j in range(both):
            here = pl.ds((b * both + j) * GROUP, GROUP)
            top = j * GROUP * MAIN
            out_ref[here, :, 0:width] = result[top : top + GROUP * MAIN].reshape(GROUP, MAIN, width)
            low = both * GROUP * MAIN + j * GROUP * EXTRA
            out_ref[here, :, width:] = folded(result[low : low + GROUP * EXTRA]).reshape(
                GROUP, MAIN, PIECE
            )
        return carry

    lax.fori_loop(0, blocks, block, 0)


def weight_kernel(pair_ref, route_ref, score_ref, main_ref, extra_ref):
    tokens = route_ref.shape[0]
    experts = main_ref.shape[1] // MAIN
    expert = iota((tokens, experts), 1)
    first, second = route_ref[:, 0:1], route_ref[:, 1:2]
    is_first, is_second = expert == first, expert == second
    hits = (is_first | is_second).astype(jnp.bfloat16)
    earlier = (iota((tokens, tokens), 0) > iota((tokens, tokens), 1)).astype(jnp.bfloat16)
    counts = dot(earlier, hits)
    group = jax.nn.sigmoid(score_ref[:, 0:1])
    pair = score_ref[:, 1:2]
    weights = (group * jax.nn.sigmoid(pair), group * jax.nn.sigmoid(-pair))
    places = []
    for mask, named in ((is_first, first), (is_second, second)):
        rank = jnp.sum(jnp.where(mask, counts, 0.0), axis=1, keepdims=True).astype(jnp.int32)
        place = member_of(named, pair_ref[0])
        places.append(
            (
                jnp.where(rank < MAIN, place * MAIN + rank, -1),
                jnp.where((rank >= MAIN) & (rank < MAIN + EXTRA), place * EXTRA + rank - MAIN, -1),
            )
        )
    for ref, which in ((main_ref, 0), (extra_ref, 1)):
        n = ref.shape[1]
        step = min(n, 256)
        for low in range(0, n, step):
            column = iota((tokens, step), 1) + low
            value = jnp.where(column == places[0][which], weights[0], 0.0)
            value = jnp.where(column == places[1][which], weights[1], value)
            ref[:, low : low + step] = value.astype(jnp.bfloat16)


def combine_kernel(back_ref, main_ref, extra_ref, out_ref, rest_ref):
    experts, _, wide = back_ref.shape
    width = wide - PIECE
    for g in range(experts // GROUP):
        block = back_ref[g * GROUP : (g + 1) * GROUP, :, width:].reshape(PIECE, PIECE)
        rest_ref[g * 2 * GROUP : (g + 1) * 2 * GROUP, :] = unfolded(block)
    step = 256

    def columns(i, carry):
        here = pl.ds(pl.multiple_of(i * step, step), step)
        rows = back_ref[:, :, here].reshape(experts * MAIN, step)
        total = dot(main_ref[...], rows) + dot(extra_ref[...], rest_ref[:, here])
        out_ref[:, here] = total.astype(jnp.bfloat16)
        return carry

    lax.fori_loop(0, width // step, columns, 0)


VMEM = pl.BlockSpec(memory_space=pltpu.VMEM)
HBM = pl.BlockSpec(memory_space=pltpu.HBM)


def in_hbm(x):
    return pltpu.with_memory_space_constraint(x, pltpu.HBM)


SMEM = pl.BlockSpec(memory_space=pltpu.SMEM)


def call(kernel, outs, ins, out_specs, scratch, limit, flops, nbytes, *args):
    return pl.pallas_call(
        kernel,
        out_shape=outs,
        in_specs=ins,
        out_specs=out_specs,
        scratch_shapes=scratch,
        compiler_params=pltpu.CompilerParams(vmem_limit_bytes=limit << 20),
        cost_estimate=pl.CostEstimate(flops=flops, bytes_accessed=nbytes, transcendentals=0),
    )(*args)


def gated_rows(value, gate):
    return (value.astype(jnp.float32) * jax.nn.sigmoid(gate.astype(jnp.float32))).astype(
        jnp.bfloat16
    )


def conv_half(conv_value, conv_gate, depth_weight, norm_gain, norm_shift, conv_out_weight):
    channels = conv_value.shape[1]
    length = conv_value.shape[0]
    first_col = lax.axis_index("tp") * channels
    taps = lax.dynamic_slice_in_dim(depth_weight, first_col, channels, 1)
    gains = lax.dynamic_slice_in_dim(norm_gain, first_col, channels, 0)
    shifts = lax.dynamic_slice_in_dim(norm_shift, first_col, channels, 0)
    reach = taps.shape[0] - 1
    last = gated_rows(conv_value[length - reach :], conv_gate[length - reach :])
    earlier = lax.ppermute(last, AXES, HALO)
    gated = gated_rows(conv_value, conv_gate)
    padded = jnp.concatenate([earlier, gated], 0).astype(jnp.float32)
    filtered = taps[0] * padded[0:length]
    for offset in range(1, reach + 1):
        filtered = filtered + taps[offset] * padded[offset : offset + length]
    sums, squares = lax.psum(
        (jnp.sum(filtered, axis=1), jnp.sum(filtered * filtered, axis=1)), "tp"
    )
    center = (sums / CONV)[:, None]
    spread = (squares / CONV)[:, None] - center * center
    normed = (filtered - center) * lax.rsqrt(spread + 1e-05) * gains + shifts
    activated = jax.nn.silu(normed).astype(jnp.bfloat16)
    partial = jnp.dot(activated, conv_out_weight, preferred_element_type=jnp.float32).astype(
        jnp.bfloat16
    )
    peers = lax.axis_size("tp")
    me = lax.axis_index("tp")
    rows = length // peers
    total = lax.dynamic_slice_in_dim(partial, me * rows, rows, 0).astype(jnp.float32)
    for by in range(1, peers):
        theirs = lax.dynamic_slice_in_dim(partial, ((me + by) % peers) * rows, rows, 0)
        came = lax.ppermute(theirs, "tp", [(i, (i + by) % peers) for i in range(peers)])
        total = total + came.astype(jnp.float32)
    return total.astype(jnp.bfloat16)


def moe_half(moe_input, moe_gain, route_experts, route_scores, expert_gate, expert_up, expert_down, conv_out):
    tokens, width = moe_input.shape
    experts = 64
    hidden = expert_gate.shape[2]
    slots = experts * (MAIN + EXTRA)
    wide = jax.ShapeDtypeStruct((experts, MAIN, width + PIECE), jnp.bfloat16)
    pair = lax.axis_index("pair").astype(jnp.int32).reshape(1)
    moved = weight_pairs()
    gate = lax.ppermute(expert_gate, AXES, moved)[0]
    up = lax.ppermute(expert_up, AXES, moved)[0]
    down = lax.ppermute(expert_down, AXES, moved)[0]
    send = call(
        send_kernel,
        pltpu.HBM(wide.shape, wide.dtype),
        [SMEM, HBM, HBM, HBM],
        HBM,
        [
            pltpu.VMEM((TOP, tokens), jnp.int32),
            pltpu.VMEM((tokens, width), jnp.bfloat16),
            pltpu.VMEM((1, width), jnp.float32),
            pltpu.VMEM((tokens, width), jnp.bfloat16),
            pltpu.VMEM((8, tokens), jnp.int32),
            pltpu.VMEM(wide.shape, jnp.bfloat16),
            pltpu.SemaphoreType.DMA((10,)),
        ],
        24,
        2 * slots * tokens * width,
        slots * width * 4,
        pair,
        in_hbm(route_experts.T),
        in_hbm(moe_input),
        in_hbm(moe_gain[None, :]),
    )
    arrived = lax.all_to_all(send, ("member", "tp"), split_axis=0, concat_axis=0, tiled=True)
    main, extra = call(
        weight_kernel,
        (
            jax.ShapeDtypeStruct((tokens, experts * MAIN), jnp.bfloat16),
            jax.ShapeDtypeStruct((tokens, experts * EXTRA), jnp.bfloat16),
        ),
        [SMEM, VMEM, VMEM],
        (VMEM, VMEM),
        [],
        16,
        2 * tokens * tokens * experts,
        4 * tokens * slots,
        pair,
        route_experts,
        route_scores,
    )
    inner = call(
        hidden_kernel,
        jax.ShapeDtypeStruct((2, slots // 2, hidden), jnp.bfloat16),
        [VMEM] * 3,
        VMEM,
        [],
        24,
        4 * slots * width * hidden,
        slots * width * 2,
        arrived,
        gate,
        up,
    )
    inner, conv_out, main, extra = lax.optimization_barrier((inner, conv_out, main, extra))
    result = call(
        down_kernel,
        wide,
        [VMEM] * 2,
        VMEM,
        [],
        24,
        2 * slots * width * hidden,
        slots * width * 2,
        inner,
        down,
    )
    returned = lax.all_to_all(result, ("member", "tp"), split_axis=0, concat_axis=0, tiled=True)
    moe_out = call(
        combine_kernel,
        jax.ShapeDtypeStruct((tokens, width), jnp.bfloat16),
        [VMEM] * 3,
        VMEM,
        [pltpu.VMEM((experts * EXTRA, width), jnp.bfloat16)],
        16,
        4 * slots * tokens * width,
        slots * width * 2,
        returned,
        main,
        extra,
    )
    return conv_out, moe_out


def on_device(
    conv_value,
    conv_gate,
    depth_weight,
    norm_gain,
    norm_shift,
    conv_out_weight,
    moe_input,
    moe_gain,
    route_experts,
    route_scores,
    expert_gate,
    expert_up,
    expert_down,
):
    conv_out = conv_half(
        conv_value, conv_gate, depth_weight, norm_gain, norm_shift, conv_out_weight
    )
    return moe_half(
        moe_input,
        moe_gain,
        route_experts,
        route_scores,
        expert_gate,
        expert_up,
        expert_down,
        conv_out,
    )


def solution(mesh):
    ep = ("pair", "member")
    every = (*ep, "tp")
    mesh = jax.sharding.Mesh(mesh.devices.reshape(4, 16, 4), every)
    in_specs = (
        P(ep, "tp"),
        P(ep, "tp"),
        P(),
        P(),
        P(),
        P("tp", None),
        P(every, None),
        P(),
        P(every, None),
        P(every, None),
        P(ep, None, None),
        P(ep, None, None),
        P(ep, None, None),
    )
    out_specs = (P(every, None), P(every, None))
    return jax.shard_map(
        on_device, mesh=mesh, in_specs=in_specs, out_specs=out_specs, check_vma=False
    )
```

```python
import jax
import jax.numpy as jnp
from jax import lax
from jax.experimental import pallas as pl
from jax.experimental.pallas import tpu as pltpu
from jax.sharding import PartitionSpec as P


CONV = 1024
TOP = 2
MAIN = 16
EXTRA = 2
PIECE = 256
PIECES = 8
GROUP = 16


AXES = ("pair", "member", "tp")
HALO = [(i, i + 4) for i in range(252)]


def iota(shape, dimension):
    return lax.broadcasted_iota(jnp.int32, shape, dimension)


def fold_matrix():
    i = iota((PIECE, PIECE), 0)
    c = iota((PIECE, PIECE), 1)
    return (c == (i % PIECES) * (2 * GROUP) + i // PIECES).astype(jnp.bfloat16)


def unfold_matrix():
    i = iota((PIECE, PIECE), 1)
    c = iota((PIECE, PIECE), 0)
    return (c == (i % PIECES) * (2 * GROUP) + i // PIECES).astype(jnp.bfloat16)


def dot(a, b):
    return jnp.dot(a, b, preferred_element_type=jnp.float32)


def folded(rows):
    stacked = jnp.concatenate([rows[:, PIECE * k : PIECE * (k + 1)] for k in range(PIECES)], 0)
    return dot(fold_matrix(), stacked).astype(jnp.bfloat16)


def unfolded(block):
    stacked = dot(unfold_matrix(), block).astype(jnp.bfloat16)
    n = 2 * GROUP
    return jnp.concatenate([stacked[n * k : n * (k + 1)] for k in range(PIECES)], 1)


def member_of(expert, pair):
    z, column, core = expert // 8, expert % 8, expert % 2
    ahead = (z - 2 * pair) % 8
    plane = ((ahead >= 1) & (ahead <= 4)).astype(jnp.int32)
    hops = jnp.where(plane == 1, ahead - 1, (8 - ahead) % 8)
    host = column + 1 - 2 * core
    return (plane * 8 + host) * 4 + jnp.where(core == 1, hops, 3 - hops)


def weight_pairs():
    pairs = []
    for device in range(256):
        z, x, core, y = device // 32, device // 8 % 4, device // 4 % 2, device % 4
        hops = y if core == 0 else 3 - y
        source = (z + hops if z % 2 else z - hops) % 8
        pairs.append((((source * 4 + x) * 2 + 1 - core) * 4 + y, device))
    return pairs


def send_kernel(pair_ref, route_in, x_in, gain_in, send_out, route_ref, x_ref, gain_ref, xn_ref, ids_ref, send_ref, sems):
    tokens, width = x_ref.shape
    experts = send_ref.shape[0]
    chunk = 96
    chunks = tokens // chunk
    loads = [
        pltpu.make_async_copy(route_in, route_ref, sems.at[0]),
        pltpu.make_async_copy(gain_in, gain_ref, sems.at[1]),
    ]
    for i in range(chunks):
        rows = pl.ds(i * chunk, chunk)
        loads.append(pltpu.make_async_copy(x_in.at[rows], x_ref.at[rows], sems.at[2 + i]))
    for load in loads:
        load.start()
    loads[0].wait()
    pair = pair_ref[0]
    expert = iota((experts, tokens), 0)
    first, second = route_ref[0:1, :], route_ref[1:2, :]
    is_first, is_second = expert == first, expert == second
    hits = (is_first | is_second).astype(jnp.bfloat16)
    earlier = (iota((tokens, tokens), 0) < iota((tokens, tokens), 1)).astype(jnp.bfloat16)
    counts = dot(hits, earlier)
    for row, (mask, named) in enumerate(((is_first, first), (is_second, second))):
        rank = jnp.sum(jnp.where(mask, counts, 0.0), axis=0, keepdims=True).astype(jnp.int32)
        place = member_of(named, pair)
        main = jnp.where(rank < MAIN, place * MAIN + rank, -1)
        extra = jnp.where((rank >= MAIN) & (rank < MAIN + EXTRA), place * EXTRA + rank - MAIN, -1)
        ids_ref[row : row + 1, :] = main
        ids_ref[row + 2 : row + 3, :] = extra
    loads[1].wait()
    step = 32
    for i in range(chunks):
        loads[2 + i].wait()

        def norm(k, carry):
            rows = pl.ds(pl.multiple_of(i * chunk + k * step, step), step)
            x = x_ref[rows, :].astype(jnp.float32)
            scale = lax.rsqrt(jnp.mean(x * x, axis=-1, keepdims=True) + 1e-06)
            xn_ref[rows, :] = (x * scale * gain_ref[...]).astype(jnp.bfloat16)
            return carry

        lax.fori_loop(0, chunk // step, norm, 0)
    stores = []
    for g in range(experts // GROUP):
        row = iota((GROUP * MAIN, tokens), 0) + g * (GROUP * MAIN)
        pick = ((row == ids_ref[0:1, :]) | (row == ids_ref[1:2, :])).astype(jnp.bfloat16)
        low = iota((GROUP * EXTRA, tokens), 0) + g * (GROUP * EXTRA)
        more = ((low == ids_ref[2:3, :]) | (low == ids_ref[3:4, :])).astype(jnp.bfloat16)
        here = pl.ds(g * GROUP, GROUP)
        send_ref[here, :, 0:width] = (
            dot(pick, xn_ref[...]).astype(jnp.bfloat16).reshape(GROUP, MAIN, width)
        )
        rest = dot(more, xn_ref[...]).astype(jnp.bfloat16)
        send_ref[here, :, width:] = folded(rest).reshape(GROUP, MAIN, PIECE)
        stores.append(pltpu.make_async_copy(send_ref.at[here], send_out.at[here], sems.at[2 + chunks + g]))
        stores[-1].start()
    for store in stores:
        store.wait()


def hidden_kernel(in_ref, gate_ref, up_ref, out_ref):
    width = gate_ref.shape[0]
    sources = in_ref.shape[0]
    both = out_ref.shape[1] // (GROUP * (MAIN + EXTRA))

    def block(b, carry):
        parts = []
        for j in range(both):
            here = pl.ds((b * both + j) * GROUP, GROUP)
            parts.append(in_ref[here, :, 0:width].reshape(GROUP * MAIN, width))
        for j in range(both):
            here = pl.ds((b * both + j) * GROUP, GROUP)
            parts.append(unfolded(in_ref[here, :, width:].reshape(PIECE, PIECE)))
        rows = jnp.concatenate(parts, 0)
        gate = dot(rows, gate_ref[...])
        up = dot(rows, up_ref[...])
        out_ref[b] = (gate / (1.0 + jnp.exp(-gate)) * up).astype(jnp.bfloat16)
        return carry

    lax.fori_loop(0, sources // (GROUP * both), block, 0)


def down_kernel(in_ref, down_ref, out_ref):
    width = down_ref.shape[1]
    blocks, rows, _ = in_ref.shape
    both = rows // (GROUP * (MAIN + EXTRA))

    def block(b, carry):
        result = dot(in_ref[b], down_ref[...]).astype(jnp.bfloat16)
        for j in range(both):
            here = pl.ds((b * both + j) * GROUP, GROUP)
            top = j * GROUP * MAIN
            out_ref[here, :, 0:width] = result[top : top + GROUP * MAIN].reshape(GROUP, MAIN, width)
            low = both * GROUP * MAIN + j * GROUP * EXTRA
            out_ref[here, :, width:] = folded(result[low : low + GROUP * EXTRA]).reshape(
                GROUP, MAIN, PIECE
            )
        return carry

    lax.fori_loop(0, blocks, block, 0)


def weight_kernel(pair_ref, route_ref, score_ref, main_ref, extra_ref):
    tokens = route_ref.shape[0]
    experts = main_ref.shape[1] // MAIN
    expert = iota((tokens, experts), 1)
    first, second = route_ref[:, 0:1], route_ref[:, 1:2]
    is_first, is_second = expert == first, expert == second
    hits = (is_first | is_second).astype(jnp.bfloat16)
    earlier = (iota((tokens, tokens), 0) > iota((tokens, tokens), 1)).astype(jnp.bfloat16)
    counts = dot(earlier, hits)
    group = jax.nn.sigmoid(score_ref[:, 0:1])
    pair = score_ref[:, 1:2]
    weights = (group * jax.nn.sigmoid(pair), group * jax.nn.sigmoid(-pair))
    places = []
    for mask, named in ((is_first, first), (is_second, second)):
        rank = jnp.sum(jnp.where(mask, counts, 0.0), axis=1, keepdims=True).astype(jnp.int32)
        place = member_of(named, pair_ref[0])
        places.append(
            (
                jnp.where(rank < MAIN, place * MAIN + rank, -1),
                jnp.where((rank >= MAIN) & (rank < MAIN + EXTRA), place * EXTRA + rank - MAIN, -1),
            )
        )
    for ref, which in ((main_ref, 0), (extra_ref, 1)):
        n = ref.shape[1]
        step = min(n, 256)
        for low in range(0, n, step):
            column = iota((tokens, step), 1) + low
            value = jnp.where(column == places[0][which], weights[0], 0.0)
            value = jnp.where(column == places[1][which], weights[1], value)
            ref[:, low : low + step] = value.astype(jnp.bfloat16)


def combine_kernel(back_ref, main_ref, extra_ref, out_ref, rest_ref):
    experts, _, wide = back_ref.shape
    width = wide - PIECE
    for g in range(experts // GROUP):
        block = back_ref[g * GROUP : (g + 1) * GROUP, :, width:].reshape(PIECE, PIECE)
        rest_ref[g * 2 * GROUP : (g + 1) * 2 * GROUP, :] = unfolded(block)
    step = 256

    def columns(i, carry):
        here = pl.ds(pl.multiple_of(i * step, step), step)
        rows = back_ref[:, :, here].reshape(experts * MAIN, step)
        total = dot(main_ref[...], rows) + dot(extra_ref[...], rest_ref[:, here])
        out_ref[:, here] = total.astype(jnp.bfloat16)
        return carry

    lax.fori_loop(0, width // step, columns, 0)


VMEM = pl.BlockSpec(memory_space=pltpu.VMEM)
HBM = pl.BlockSpec(memory_space=pltpu.HBM)


def in_hbm(x):
    return pltpu.with_memory_space_constraint(x, pltpu.HBM)


SMEM = pl.BlockSpec(memory_space=pltpu.SMEM)


def call(kernel, outs, ins, out_specs, scratch, limit, flops, nbytes, *args):
    return pl.pallas_call(
        kernel,
        out_shape=outs,
        in_specs=ins,
        out_specs=out_specs,
        scratch_shapes=scratch,
        compiler_params=pltpu.CompilerParams(vmem_limit_bytes=limit << 20),
        cost_estimate=pl.CostEstimate(flops=flops, bytes_accessed=nbytes, transcendentals=0),
    )(*args)


def gated_rows(value, gate):
    return (value.astype(jnp.float32) * jax.nn.sigmoid(gate.astype(jnp.float32))).astype(
        jnp.bfloat16
    )


def conv_kernel(me_ref, b0, b1, b2, b3, taps_ref, gain_ref, shift_ref, w0, w1, w2, w3, out_ref, x_ref, f_ref):
    halves, rows, lanes = f_ref.shape
    blocks = (b0, b1, b2, b3)
    peers = len(blocks)
    taps = taps_ref.shape[0]
    lead = b0.shape[0] - rows - (taps - 1)
    me = me_ref[0]
    for k, block in enumerate(blocks):
        x_ref[2 * k] = block[:, :lanes].astype(jnp.float32)
        x_ref[2 * k + 1] = block[:, lanes:].astype(jnp.float32)

    def columns(i):
        source = (me + peers - i // 2) % peers
        return pl.ds(pl.multiple_of((source * 2 + i % 2) * lanes, lanes), lanes)

    step = 64

    def filtered(i, carry):
        cols = columns(i)
        total, squares = carry
        sums, sums2 = [], []
        for base in range(0, rows, step):
            value = taps_ref[0:1, cols] * x_ref[i, base + lead : base + lead + step, :]
            for j in range(1, taps):
                low = base + lead + j
                value = value + taps_ref[j : j + 1, cols] * x_ref[i, low : low + step, :]
            f_ref[i, base : base + step, :] = value
            sums.append(value)
            sums2.append(value * value)
        return total + jnp.concatenate(sums, 0), squares + jnp.concatenate(sums2, 0)

    zero = jnp.zeros((rows, lanes), jnp.float32)
    total, squares = lax.fori_loop(0, halves, filtered, (zero, zero))
    center = jnp.sum(total, axis=1, keepdims=True) / CONV
    spread = jnp.sum(squares, axis=1, keepdims=True) / CONV - center * center
    scale = lax.rsqrt(spread + 1e-05)
    acts = []
    for i in range(halves):
        cols = columns(i)
        normed = (f_ref[i] - center) * scale * gain_ref[:, cols] + shift_ref[:, cols]
        acts.append((normed / (1.0 + jnp.exp(-normed))).astype(jnp.bfloat16))
    acts = [jnp.concatenate(acts[2 * k : 2 * k + 2], 1) for k in range(peers)]
    width = 512
    for low in range(0, out_ref.shape[1], width):
        summed = jnp.zeros((rows, width), jnp.float32)
        for act, weight in zip(acts, (w0, w1, w2, w3)):
            partial = dot(act, weight[:, low : low + width]).astype(jnp.bfloat16)
            summed = summed + partial.astype(jnp.float32)
        out_ref[:, low : low + width] = summed.astype(jnp.bfloat16)


def conv_half(conv_value, conv_gate, depth_weight, norm_gain, norm_shift, conv_out_weight):
    length, channels = conv_value.shape
    peers = lax.axis_size("tp")
    me = lax.axis_index("tp").astype(jnp.int32)
    rows = length // peers
    reach = 32
    last = gated_rows(conv_value[length - reach :], conv_gate[length - reach :])
    earlier = lax.ppermute(last, AXES, HALO)
    padded = jnp.concatenate([earlier, gated_rows(conv_value, conv_gate)], 0)
    blocks, weights = [], []
    for by in range(peers):
        peer = (me + by) % peers
        block = lax.dynamic_slice_in_dim(padded, peer * rows, rows + reach, 0)
        weight = conv_out_weight
        if by > 0:
            ring = [(i, (i + by) % peers) for i in range(peers)]
            block = lax.ppermute(block, "tp", ring)
            weight = lax.ppermute(weight, "tp", ring)
        blocks.append(block)
        weights.append(weight)
    width = conv_out_weight.shape[1]
    return call(
        conv_kernel,
        jax.ShapeDtypeStruct((rows, width), jnp.bfloat16),
        [SMEM] + [VMEM] * 11,
        VMEM,
        [
            pltpu.VMEM((2 * peers, rows + reach, channels // 2), jnp.float32),
            pltpu.VMEM((2 * peers, rows, channels // 2), jnp.float32),
        ],
        24,
        2 * rows * CONV * width,
        CONV * width * 2,
        me.reshape(1),
        *blocks,
        depth_weight,
        norm_gain[None, :],
        norm_shift[None, :],
        *weights,
    )


def moe_half(moe_input, moe_gain, route_experts, route_scores, expert_gate, expert_up, expert_down, conv_out):
    tokens, width = moe_input.shape
    experts = 64
    hidden = expert_gate.shape[2]
    slots = experts * (MAIN + EXTRA)
    wide = jax.ShapeDtypeStruct((experts, MAIN, width + PIECE), jnp.bfloat16)
    pair = lax.axis_index("pair").astype(jnp.int32).reshape(1)
    moved = weight_pairs()
    gate = lax.ppermute(expert_gate, AXES, moved)[0]
    up = lax.ppermute(expert_up, AXES, moved)[0]
    down = lax.ppermute(expert_down, AXES, moved)[0]
    send = call(
        send_kernel,
        pltpu.HBM(wide.shape, wide.dtype),
        [SMEM, HBM, HBM, HBM],
        HBM,
        [
            pltpu.VMEM((TOP, tokens), jnp.int32),
            pltpu.VMEM((tokens, width), jnp.bfloat16),
            pltpu.VMEM((1, width), jnp.float32),
            pltpu.VMEM((tokens, width), jnp.bfloat16),
            pltpu.VMEM((8, tokens), jnp.int32),
            pltpu.VMEM(wide.shape, jnp.bfloat16),
            pltpu.SemaphoreType.DMA((10,)),
        ],
        24,
        2 * slots * tokens * width,
        slots * width * 4,
        pair,
        in_hbm(route_experts.T),
        in_hbm(moe_input),
        in_hbm(moe_gain[None, :]),
    )
    arrived = lax.all_to_all(send, ("member", "tp"), split_axis=0, concat_axis=0, tiled=True)
    main, extra = call(
        weight_kernel,
        (
            jax.ShapeDtypeStruct((tokens, experts * MAIN), jnp.bfloat16),
            jax.ShapeDtypeStruct((tokens, experts * EXTRA), jnp.bfloat16),
        ),
        [SMEM, VMEM, VMEM],
        (VMEM, VMEM),
        [],
        16,
        2 * tokens * tokens * experts,
        4 * tokens * slots,
        pair,
        route_experts,
        route_scores,
    )
    inner = call(
        hidden_kernel,
        jax.ShapeDtypeStruct((2, slots // 2, hidden), jnp.bfloat16),
        [VMEM] * 3,
        VMEM,
        [],
        24,
        4 * slots * width * hidden,
        slots * width * 2,
        arrived,
        gate,
        up,
    )
    inner, conv_out, main, extra = lax.optimization_barrier((inner, conv_out, main, extra))
    result = call(
        down_kernel,
        wide,
        [VMEM] * 2,
        VMEM,
        [],
        24,
        2 * slots * width * hidden,
        slots * width * 2,
        inner,
        down,
    )
    returned = lax.all_to_all(result, ("member", "tp"), split_axis=0, concat_axis=0, tiled=True)
    moe_out = call(
        combine_kernel,
        jax.ShapeDtypeStruct((tokens, width), jnp.bfloat16),
        [VMEM] * 3,
        VMEM,
        [pltpu.VMEM((experts * EXTRA, width), jnp.bfloat16)],
        16,
        4 * slots * tokens * width,
        slots * width * 2,
        returned,
        main,
        extra,
    )
    return conv_out, moe_out


def on_device(
    conv_value,
    conv_gate,
    depth_weight,
    norm_gain,
    norm_shift,
    conv_out_weight,
    moe_input,
    moe_gain,
    route_experts,
    route_scores,
    expert_gate,
    expert_up,
    expert_down,
):
    conv_out = conv_half(
        conv_value, conv_gate, depth_weight, norm_gain, norm_shift, conv_out_weight
    )
    return moe_half(
        moe_input,
        moe_gain,
        route_experts,
        route_scores,
        expert_gate,
        expert_up,
        expert_down,
        conv_out,
    )


def solution(mesh):
    ep = ("pair", "member")
    every = (*ep, "tp")
    mesh = jax.sharding.Mesh(mesh.devices.reshape(4, 16, 4), every)
    in_specs = (
        P(ep, "tp"),
        P(ep, "tp"),
        P(),
        P(),
        P(),
        P("tp", None),
        P(every, None),
        P(),
        P(every, None),
        P(every, None),
        P(ep, None, None),
        P(ep, None, None),
        P(ep, None, None),
    )
    out_specs = (P(every, None), P(every, None))
    return jax.shard_map(
        on_device, mesh=mesh, in_specs=in_specs, out_specs=out_specs, check_vma=False
    )
```

```python
import jax
import jax.numpy as jnp
from jax import lax
from jax.experimental import pallas as pl
from jax.experimental.pallas import tpu as pltpu
from jax.sharding import PartitionSpec as P


CONV = 1024
TOP = 2
MAIN = 16
EXTRA = 2
PIECE = 256
PIECES = 8
GROUP = 16
LEFT = 768


AXES = ("pair", "member", "tp")
HALO = [(i, i + 4) for i in range(252)]


def iota(shape, dimension):
    return lax.broadcasted_iota(jnp.int32, shape, dimension)


def fold_matrix():
    i = iota((PIECE, PIECE), 0)
    c = iota((PIECE, PIECE), 1)
    return (c == (i % PIECES) * (2 * GROUP) + i // PIECES).astype(jnp.bfloat16)


def unfold_matrix():
    i = iota((PIECE, PIECE), 1)
    c = iota((PIECE, PIECE), 0)
    return (c == (i % PIECES) * (2 * GROUP) + i // PIECES).astype(jnp.bfloat16)


def dot(a, b):
    return jnp.dot(a, b, preferred_element_type=jnp.float32)


def folded(rows):
    stacked = jnp.concatenate([rows[:, PIECE * k : PIECE * (k + 1)] for k in range(PIECES)], 0)
    return dot(fold_matrix(), stacked).astype(jnp.bfloat16)


def unfolded(block):
    stacked = dot(unfold_matrix(), block).astype(jnp.bfloat16)
    n = 2 * GROUP
    return jnp.concatenate([stacked[n * k : n * (k + 1)] for k in range(PIECES)], 1)


def member_of(expert, pair):
    z, column, core = expert // 8, expert % 8, expert % 2
    ahead = (z - 2 * pair) % 8
    plane = ((ahead >= 1) & (ahead <= 4)).astype(jnp.int32)
    hops = jnp.where(plane == 1, ahead - 1, (8 - ahead) % 8)
    host = column + 1 - 2 * core
    return (plane * 8 + host) * 4 + jnp.where(core == 1, hops, 3 - hops)


def weight_pairs():
    pairs = []
    for device in range(256):
        z, x, core, y = device // 32, device // 8 % 4, device // 4 % 2, device % 4
        hops = y if core == 0 else 3 - y
        source = (z + hops if z % 2 else z - hops) % 8
        pairs.append((((source * 4 + x) * 2 + 1 - core) * 4 + y, device))
    return pairs


def send_kernel(pair_ref, route_in, x_in, gain_in, send_out, route_ref, x_ref, gain_ref, xn_ref, ids_ref, send_ref, sems):
    tokens, width = x_ref.shape
    experts = send_ref.shape[0]
    chunk = 96
    chunks = tokens // chunk
    loads = [
        pltpu.make_async_copy(route_in, route_ref, sems.at[0]),
        pltpu.make_async_copy(gain_in, gain_ref, sems.at[1]),
    ]
    for i in range(chunks):
        rows = pl.ds(i * chunk, chunk)
        loads.append(pltpu.make_async_copy(x_in.at[rows], x_ref.at[rows], sems.at[2 + i]))
    for load in loads:
        load.start()
    loads[0].wait()
    pair = pair_ref[0]
    expert = iota((experts, tokens), 0)
    first, second = route_ref[0:1, :], route_ref[1:2, :]
    is_first, is_second = expert == first, expert == second
    hits = (is_first | is_second).astype(jnp.bfloat16)
    earlier = (iota((tokens, tokens), 0) < iota((tokens, tokens), 1)).astype(jnp.bfloat16)
    counts = dot(hits, earlier)
    for row, (mask, named) in enumerate(((is_first, first), (is_second, second))):
        rank = jnp.sum(jnp.where(mask, counts, 0.0), axis=0, keepdims=True).astype(jnp.int32)
        place = member_of(named, pair)
        main = jnp.where(rank < MAIN, place * MAIN + rank, -1)
        extra = jnp.where((rank >= MAIN) & (rank < MAIN + EXTRA), place * EXTRA + rank - MAIN, -1)
        ids_ref[row : row + 1, :] = main
        ids_ref[row + 2 : row + 3, :] = extra
    loads[1].wait()
    step = 32
    for i in range(chunks):
        loads[2 + i].wait()

        def norm(k, carry):
            rows = pl.ds(pl.multiple_of(i * chunk + k * step, step), step)
            x = x_ref[rows, :].astype(jnp.float32)
            scale = lax.rsqrt(jnp.mean(x * x, axis=-1, keepdims=True) + 1e-06)
            xn_ref[rows, :] = (x * scale * gain_ref[...]).astype(jnp.bfloat16)
            return carry

        lax.fori_loop(0, chunk // step, norm, 0)
    stores = []
    for g in range(experts // GROUP):
        row = iota((GROUP * MAIN, tokens), 0) + g * (GROUP * MAIN)
        pick = ((row == ids_ref[0:1, :]) | (row == ids_ref[1:2, :])).astype(jnp.bfloat16)
        low = iota((GROUP * EXTRA, tokens), 0) + g * (GROUP * EXTRA)
        more = ((low == ids_ref[2:3, :]) | (low == ids_ref[3:4, :])).astype(jnp.bfloat16)
        here = pl.ds(g * GROUP, GROUP)
        send_ref[here, :, 0:width] = (
            dot(pick, xn_ref[...]).astype(jnp.bfloat16).reshape(GROUP, MAIN, width)
        )
        rest = dot(more, xn_ref[...]).astype(jnp.bfloat16)
        send_ref[here, :, width:] = folded(rest).reshape(GROUP, MAIN, PIECE)
        stores.append(pltpu.make_async_copy(send_ref.at[here], send_out.at[here], sems.at[2 + chunks + g]))
        stores[-1].start()
    for store in stores:
        store.wait()


def hidden_kernel(in_ref, gate_ref, up_ref, out_ref):
    width = gate_ref.shape[0]
    sources = in_ref.shape[0]
    both = out_ref.shape[1] // (GROUP * (MAIN + EXTRA))

    def block(b, carry):
        parts = []
        for j in range(both):
            here = pl.ds((b * both + j) * GROUP, GROUP)
            parts.append(in_ref[here, :, 0:width].reshape(GROUP * MAIN, width))
        for j in range(both):
            here = pl.ds((b * both + j) * GROUP, GROUP)
            parts.append(unfolded(in_ref[here, :, width:].reshape(PIECE, PIECE)))
        rows = jnp.concatenate(parts, 0)
        gate = dot(rows, gate_ref[...])
        up = dot(rows, up_ref[...])
        out_ref[b] = (gate / (1.0 + jnp.exp(-gate)) * up).astype(jnp.bfloat16)
        return carry

    lax.fori_loop(0, sources // (GROUP * both), block, 0)


def left_kernel(in_ref, left_ref, out_ref):
    blocks, rows, _ = in_ref.shape
    both = rows // (GROUP * (MAIN + EXTRA))
    main = both * GROUP * MAIN

    def block(b, carry):
        here = pl.ds(b * both * GROUP, both * GROUP)
        result = dot(in_ref[b, :main, :], left_ref[...]).astype(jnp.bfloat16)
        out_ref[here, :, :] = result.reshape(both * GROUP, MAIN, out_ref.shape[2])
        return carry

    lax.fori_loop(0, blocks, block, 0)


def right_kernel(in_ref, left_ref, right_ref, out_ref):
    width = right_ref.shape[1]
    blocks, rows, _ = in_ref.shape
    both = rows // (GROUP * (MAIN + EXTRA))
    main = both * GROUP * MAIN

    def block(b, carry):
        here = pl.ds(b * both * GROUP, both * GROUP)
        result = dot(in_ref[b], right_ref[...]).astype(jnp.bfloat16)
        out_ref[here, :, 0:width] = result[:main].reshape(both * GROUP, MAIN, width)
        start = dot(in_ref[b, main:, :], left_ref[...]).astype(jnp.bfloat16)
        rest = jnp.concatenate([start, result[main:]], 1)
        for j in range(both):
            there = pl.ds((b * both + j) * GROUP, GROUP)
            piece = folded(rest[j * GROUP * EXTRA : (j + 1) * GROUP * EXTRA])
            out_ref[there, :, width:] = piece.reshape(GROUP, MAIN, PIECE)
        return carry

    lax.fori_loop(0, blocks, block, 0)


def weight_kernel(pair_ref, route_ref, score_ref, main_ref, extra_ref):
    tokens = route_ref.shape[0]
    experts = main_ref.shape[1] // MAIN
    expert = iota((tokens, experts), 1)
    first, second = route_ref[:, 0:1], route_ref[:, 1:2]
    is_first, is_second = expert == first, expert == second
    hits = (is_first | is_second).astype(jnp.bfloat16)
    earlier = (iota((tokens, tokens), 0) > iota((tokens, tokens), 1)).astype(jnp.bfloat16)
    counts = dot(earlier, hits)
    group = jax.nn.sigmoid(score_ref[:, 0:1])
    pair = score_ref[:, 1:2]
    weights = (group * jax.nn.sigmoid(pair), group * jax.nn.sigmoid(-pair))
    places = []
    for mask, named in ((is_first, first), (is_second, second)):
        rank = jnp.sum(jnp.where(mask, counts, 0.0), axis=1, keepdims=True).astype(jnp.int32)
        place = member_of(named, pair_ref[0])
        places.append(
            (
                jnp.where(rank < MAIN, place * MAIN + rank, -1),
                jnp.where((rank >= MAIN) & (rank < MAIN + EXTRA), place * EXTRA + rank - MAIN, -1),
            )
        )
    for ref, which in ((main_ref, 0), (extra_ref, 1)):
        n = ref.shape[1]
        step = min(n, 256)
        for low in range(0, n, step):
            column = iota((tokens, step), 1) + low
            value = jnp.where(column == places[0][which], weights[0], 0.0)
            value = jnp.where(column == places[1][which], weights[1], value)
            ref[:, low : low + step] = value.astype(jnp.bfloat16)


def combine_kernel(left_ref, right_ref, main_ref, extra_ref, out_ref, rest_ref):
    experts, _, start = left_ref.shape
    width = right_ref.shape[2] - PIECE
    for g in range(experts // GROUP):
        block = right_ref[g * GROUP : (g + 1) * GROUP, :, width:].reshape(PIECE, PIECE)
        rest_ref[g * 2 * GROUP : (g + 1) * 2 * GROUP, :] = unfolded(block)
    step = 256
    for ref, first, count in ((left_ref, 0, start), (right_ref, start, width)):

        def columns(i, carry):
            here = pl.ds(pl.multiple_of(i * step, step), step)
            there = pl.ds(pl.multiple_of(first + i * step, step), step)
            rows = ref[:, :, here].reshape(experts * MAIN, step)
            total = dot(main_ref[...], rows) + dot(extra_ref[...], rest_ref[:, there])
            out_ref[:, there] = total.astype(jnp.bfloat16)
            return carry

        lax.fori_loop(0, count // step, columns, 0)


VMEM = pl.BlockSpec(memory_space=pltpu.VMEM)
HBM = pl.BlockSpec(memory_space=pltpu.HBM)


def in_hbm(x):
    return pltpu.with_memory_space_constraint(x, pltpu.HBM)


SMEM = pl.BlockSpec(memory_space=pltpu.SMEM)


def call(kernel, outs, ins, out_specs, scratch, limit, flops, nbytes, *args):
    return pl.pallas_call(
        kernel,
        out_shape=outs,
        in_specs=ins,
        out_specs=out_specs,
        scratch_shapes=scratch,
        compiler_params=pltpu.CompilerParams(vmem_limit_bytes=limit << 20),
        cost_estimate=pl.CostEstimate(flops=flops, bytes_accessed=nbytes, transcendentals=0),
    )(*args)


def gated_rows(value, gate):
    return (value.astype(jnp.float32) * jax.nn.sigmoid(gate.astype(jnp.float32))).astype(
        jnp.bfloat16
    )


def conv_kernel(
    me_ref, b0, b1, b2, b3, taps_ref, gain_ref, shift_ref, own, m1, m2, m3, o1, o2, o3, out_ref, x_ref, f_ref
):
    halves, rows, lanes = f_ref.shape
    blocks = (b0, b1, b2, b3)
    peers = len(blocks)
    taps = taps_ref.shape[0]
    lead = b0.shape[0] - rows - (taps - 1)
    me, core = me_ref[0], me_ref[1]
    parts = [pl.ds(pl.multiple_of(h * lanes, lanes), lanes) for h in (core, 1 - core)]
    for k, block in enumerate(blocks):
        for h, part in enumerate(parts):
            x_ref[2 * k + h] = block[:, part].astype(jnp.float32)

    def columns(i):
        source = (me + peers - i // 2) % peers
        half = (core + i) % 2
        return pl.ds(pl.multiple_of((source * 2 + half) * lanes, lanes), lanes)

    step = 64

    def filtered(i, carry):
        cols = columns(i)
        total, squares = carry
        sums, sums2 = [], []
        for base in range(0, rows, step):
            value = taps_ref[0:1, cols] * x_ref[i, base + lead : base + lead + step, :]
            for j in range(1, taps):
                low = base + lead + j
                value = value + taps_ref[j : j + 1, cols] * x_ref[i, low : low + step, :]
            f_ref[i, base : base + step, :] = value
            sums.append(value)
            sums2.append(value * value)
        return total + jnp.concatenate(sums, 0), squares + jnp.concatenate(sums2, 0)

    zero = jnp.zeros((rows, lanes), jnp.float32)
    total, squares = lax.fori_loop(0, halves, filtered, (zero, zero))
    center = jnp.sum(total, axis=1, keepdims=True) / CONV
    spread = jnp.sum(squares, axis=1, keepdims=True) / CONV - center * center
    scale = lax.rsqrt(spread + 1e-05)
    acts = []
    for i in range(halves):
        cols = columns(i)
        normed = (f_ref[i] - center) * scale * gain_ref[:, cols] + shift_ref[:, cols]
        acts.append((normed / (1.0 + jnp.exp(-normed))).astype(jnp.bfloat16))
    acts = [jnp.concatenate(acts[2 * k : 2 * k + 2], 1) for k in range(peers)]
    width = 512
    for low in range(0, out_ref.shape[1], width):
        summed = jnp.zeros((rows, width), jnp.float32)
        cols = slice(low, low + width)
        pairs = [(own[parts[0], cols], own[parts[1], cols])]
        pairs += [(m[:, cols], o[:, cols]) for m, o in ((m1, o1), (m2, o2), (m3, o3))]
        for act, weight in zip(acts, pairs):
            partial = dot(act, jnp.concatenate(weight, 0)).astype(jnp.bfloat16)
            summed = summed + partial.astype(jnp.float32)
        out_ref[:, low : low + width] = summed.astype(jnp.bfloat16)


def conv_half(conv_value, conv_gate, depth_weight, norm_gain, norm_shift, conv_out_weight):
    length, channels = conv_value.shape
    peers = lax.axis_size("tp")
    me = lax.axis_index("tp").astype(jnp.int32)
    rows = length // peers
    reach = 32
    last = gated_rows(conv_value[length - reach :], conv_gate[length - reach :])
    earlier = lax.ppermute(last, AXES, HALO)
    padded = jnp.concatenate([earlier, gated_rows(conv_value, conv_gate)], 0)
    core = lax.axis_index("member").astype(jnp.int32) % 2
    half = channels // 2
    part = lax.dynamic_slice_in_dim(conv_out_weight, core * half, half, 0)
    blocks, mine, others = [], [], []
    for by in range(peers):
        peer = (me + by) % peers
        block = lax.dynamic_slice_in_dim(padded, peer * rows, rows + reach, 0)
        if by > 0:
            ring = [(i, (i + by) % peers) for i in range(peers)]
            block = lax.ppermute(block, "tp", ring)
            mine.append(lax.ppermute(part, "tp", ring))
            others.append(lax.ppermute(mine[-1], AXES, [(i, i ^ 4) for i in range(256)]))
        blocks.append(block)
    width = conv_out_weight.shape[1]
    return call(
        conv_kernel,
        jax.ShapeDtypeStruct((rows, width), jnp.bfloat16),
        [SMEM] + [VMEM] * 14,
        VMEM,
        [
            pltpu.VMEM((2 * peers, rows + reach, channels // 2), jnp.float32),
            pltpu.VMEM((2 * peers, rows, channels // 2), jnp.float32),
        ],
        24,
        2 * rows * CONV * width,
        CONV * width * 2,
        jnp.stack([me, core]),
        *blocks,
        depth_weight,
        norm_gain[None, :],
        norm_shift[None, :],
        conv_out_weight,
        *mine,
        *others,
    )


def moe_half(moe_input, moe_gain, route_experts, route_scores, expert_gate, expert_up, expert_down, conv_out):
    tokens, width = moe_input.shape
    experts = 64
    hidden = expert_gate.shape[2]
    slots = experts * (MAIN + EXTRA)
    wide = jax.ShapeDtypeStruct((experts, MAIN, width + PIECE), jnp.bfloat16)
    pair = lax.axis_index("pair").astype(jnp.int32).reshape(1)
    moved = weight_pairs()
    gate = lax.ppermute(expert_gate, AXES, moved)[0]
    up = lax.ppermute(expert_up, AXES, moved)[0]
    left = lax.ppermute(expert_down[:, :, :LEFT], AXES, moved)[0]
    right = lax.ppermute(expert_down[:, :, LEFT:], AXES, moved)[0]
    send = call(
        send_kernel,
        pltpu.HBM(wide.shape, wide.dtype),
        [SMEM, HBM, HBM, HBM],
        HBM,
        [
            pltpu.VMEM((TOP, tokens), jnp.int32),
            pltpu.VMEM((tokens, width), jnp.bfloat16),
            pltpu.VMEM((1, width), jnp.float32),
            pltpu.VMEM((tokens, width), jnp.bfloat16),
            pltpu.VMEM((8, tokens), jnp.int32),
            pltpu.VMEM(wide.shape, jnp.bfloat16),
            pltpu.SemaphoreType.DMA((10,)),
        ],
        24,
        2 * slots * tokens * width,
        slots * width * 4,
        pair,
        in_hbm(route_experts.T),
        in_hbm(moe_input),
        in_hbm(moe_gain[None, :]),
    )
    arrived = lax.all_to_all(send, ("member", "tp"), split_axis=0, concat_axis=0, tiled=True)
    main, extra = call(
        weight_kernel,
        (
            jax.ShapeDtypeStruct((tokens, experts * MAIN), jnp.bfloat16),
            jax.ShapeDtypeStruct((tokens, experts * EXTRA), jnp.bfloat16),
        ),
        [SMEM, VMEM, VMEM],
        (VMEM, VMEM),
        [],
        16,
        2 * tokens * tokens * experts,
        4 * tokens * slots,
        pair,
        route_experts,
        route_scores,
    )
    inner = call(
        hidden_kernel,
        jax.ShapeDtypeStruct((2, slots // 2, hidden), jnp.bfloat16),
        [VMEM] * 3,
        VMEM,
        [],
        24,
        4 * slots * width * hidden,
        slots * width * 2,
        arrived,
        gate,
        up,
    )
    inner, conv_out, main, extra = lax.optimization_barrier((inner, conv_out, main, extra))
    first = call(
        left_kernel,
        jax.ShapeDtypeStruct((experts, MAIN, LEFT), jnp.bfloat16),
        [VMEM] * 2,
        VMEM,
        [],
        16,
        2 * slots * LEFT * hidden,
        slots * LEFT * 2,
        inner,
        left,
    )
    back1 = lax.all_to_all(first, ("member", "tp"), split_axis=0, concat_axis=0, tiled=True)
    inner, back1 = lax.optimization_barrier((inner, back1))
    second = call(
        right_kernel,
        jax.ShapeDtypeStruct((experts, MAIN, width - LEFT + PIECE), jnp.bfloat16),
        [VMEM] * 3,
        VMEM,
        [],
        16,
        2 * slots * (width - LEFT) * hidden,
        slots * width * 2,
        inner,
        left,
        right,
    )
    back2 = lax.all_to_all(second, ("member", "tp"), split_axis=0, concat_axis=0, tiled=True)
    moe_out = call(
        combine_kernel,
        jax.ShapeDtypeStruct((tokens, width), jnp.bfloat16),
        [VMEM] * 4,
        VMEM,
        [pltpu.VMEM((experts * EXTRA, width), jnp.bfloat16)],
        16,
        2 * slots * tokens * width,
        slots * width * 2,
        back1,
        back2,
        main,
        extra,
    )
    return conv_out, moe_out


def on_device(
    conv_value,
    conv_gate,
    depth_weight,
    norm_gain,
    norm_shift,
    conv_out_weight,
    moe_input,
    moe_gain,
    route_experts,
    route_scores,
    expert_gate,
    expert_up,
    expert_down,
):
    conv_out = conv_half(
        conv_value, conv_gate, depth_weight, norm_gain, norm_shift, conv_out_weight
    )
    return moe_half(
        moe_input,
        moe_gain,
        route_experts,
        route_scores,
        expert_gate,
        expert_up,
        expert_down,
        conv_out,
    )


def solution(mesh):
    ep = ("pair", "member")
    every = (*ep, "tp")
    mesh = jax.sharding.Mesh(mesh.devices.reshape(4, 16, 4), every)
    in_specs = (
        P(ep, "tp"),
        P(ep, "tp"),
        P(),
        P(),
        P(),
        P("tp", None),
        P(every, None),
        P(),
        P(every, None),
        P(every, None),
        P(ep, None, None),
        P(ep, None, None),
        P(ep, None, None),
    )
    out_specs = (P(every, None), P(every, None))
    return jax.shard_map(
        on_device, mesh=mesh, in_specs=in_specs, out_specs=out_specs, check_vma=False
    )
```

```python
import jax
import jax.numpy as jnp
from jax import lax
from jax.experimental import pallas as pl
from jax.experimental.pallas import tpu as pltpu
from jax.sharding import PartitionSpec as P


CONV = 1024
TOP = 2
MAIN = 16
EXTRA = 2
PIECE = 256
PIECES = 8
GROUP = 16
LEFT = 768


AXES = ("pair", "member", "tp")
HALO = [(i, i + 4) for i in range(252)]


def iota(shape, dimension):
    return lax.broadcasted_iota(jnp.int32, shape, dimension)


def fold_matrix():
    i = iota((PIECE, PIECE), 0)
    c = iota((PIECE, PIECE), 1)
    return (c == (i % PIECES) * (2 * GROUP) + i // PIECES).astype(jnp.bfloat16)


def unfold_matrix():
    i = iota((PIECE, PIECE), 1)
    c = iota((PIECE, PIECE), 0)
    return (c == (i % PIECES) * (2 * GROUP) + i // PIECES).astype(jnp.bfloat16)


def dot(a, b):
    return jnp.dot(a, b, preferred_element_type=jnp.float32)


def folded(rows):
    stacked = jnp.concatenate([rows[:, PIECE * k : PIECE * (k + 1)] for k in range(PIECES)], 0)
    return dot(fold_matrix(), stacked).astype(jnp.bfloat16)


def unfolded(block):
    stacked = dot(unfold_matrix(), block).astype(jnp.bfloat16)
    n = 2 * GROUP
    return jnp.concatenate([stacked[n * k : n * (k + 1)] for k in range(PIECES)], 1)


def member_of(expert, pair):
    z, x, core = expert // 8, expert // 2 % 4, expert % 2
    ahead = (z - 2 * pair) % 8
    plane = ((ahead >= 1) & (ahead <= 4)).astype(jnp.int32)
    hops = jnp.where(plane == 1, ahead - 1, (8 - ahead) % 8)
    y = 2 * core + jnp.where(hops == 2, 1, jnp.where(hops == 0, 3 - 4 * core, 0))
    host = jnp.where(hops == 3, 1 - core, core)
    return (plane * 8 + x * 2 + host) * 4 + y


def hops_of(y, core):
    return 1 + y % 2 + jnp.where(core == y // 2, 0, jnp.where(y % 2 == 1, -2, 2))


def weight_pairs(array):
    pairs = []
    for device in range(256):
        z, x, core, y = device // 32, device // 8 % 4, device // 4 % 2, device % 4
        hops = {(0, 0): 1, (1, 0): 3, (0, 1): 2, (1, 1): 0, (1, 2): 1, (0, 2): 3, (1, 3): 2, (0, 3): 0}[core, y]
        owner = 1 - core if hops == 3 else core
        back = 1 if z % 2 else -1
        if array == "relay":
            if hops == 3:
                pairs.append((z + 2 * back, x, owner, y, device))
        elif hops in (1, 2):
            pairs.append((z + hops * back, x, owner, y ^ 1 if array == "gate" else y, device))
        elif hops == 3 and array == "gate":
            pairs.append((z + 3 * back, x, owner, 3 - y, device))
    return [(((z % 8 * 4 + x) * 2 + core) * 4 + y, device) for z, x, core, y, device in pairs]


def send_kernel(pair_ref, route_in, x_in, gain_in, send_out, route_ref, x_ref, gain_ref, xn_ref, ids_ref, send_ref, sems):
    tokens, width = x_ref.shape
    experts = send_ref.shape[0]
    chunk = 96
    chunks = tokens // chunk
    loads = [
        pltpu.make_async_copy(route_in, route_ref, sems.at[0]),
        pltpu.make_async_copy(gain_in, gain_ref, sems.at[1]),
    ]
    for i in range(chunks):
        rows = pl.ds(i * chunk, chunk)
        loads.append(pltpu.make_async_copy(x_in.at[rows], x_ref.at[rows], sems.at[2 + i]))
    for load in loads:
        load.start()
    loads[0].wait()
    pair = pair_ref[0]
    expert = iota((experts, tokens), 0)
    first, second = route_ref[0:1, :], route_ref[1:2, :]
    is_first, is_second = expert == first, expert == second
    hits = (is_first | is_second).astype(jnp.bfloat16)
    earlier = (iota((tokens, tokens), 0) < iota((tokens, tokens), 1)).astype(jnp.bfloat16)
    counts = dot(hits, earlier)
    for row, (mask, named) in enumerate(((is_first, first), (is_second, second))):
        rank = jnp.sum(jnp.where(mask, counts, 0.0), axis=0, keepdims=True).astype(jnp.int32)
        place = member_of(named, pair)
        main = jnp.where(rank < MAIN, place * MAIN + rank, -1)
        extra = jnp.where((rank >= MAIN) & (rank < MAIN + EXTRA), place * EXTRA + rank - MAIN, -1)
        ids_ref[row : row + 1, :] = main
        ids_ref[row + 2 : row + 3, :] = extra
    loads[1].wait()
    step = 32
    for i in range(chunks):
        loads[2 + i].wait()

        def norm(k, carry):
            rows = pl.ds(pl.multiple_of(i * chunk + k * step, step), step)
            x = x_ref[rows, :].astype(jnp.float32)
            scale = lax.rsqrt(jnp.mean(x * x, axis=-1, keepdims=True) + 1e-06)
            xn_ref[rows, :] = (x * scale * gain_ref[...]).astype(jnp.bfloat16)
            return carry

        lax.fori_loop(0, chunk // step, norm, 0)
    stores = []
    for g in range(experts // GROUP):
        row = iota((GROUP * MAIN, tokens), 0) + g * (GROUP * MAIN)
        pick = ((row == ids_ref[0:1, :]) | (row == ids_ref[1:2, :])).astype(jnp.bfloat16)
        low = iota((GROUP * EXTRA, tokens), 0) + g * (GROUP * EXTRA)
        more = ((low == ids_ref[2:3, :]) | (low == ids_ref[3:4, :])).astype(jnp.bfloat16)
        here = pl.ds(g * GROUP, GROUP)
        send_ref[here, :, 0:width] = (
            dot(pick, xn_ref[...]).astype(jnp.bfloat16).reshape(GROUP, MAIN, width)
        )
        rest = dot(more, xn_ref[...]).astype(jnp.bfloat16)
        send_ref[here, :, width:] = folded(rest).reshape(GROUP, MAIN, PIECE)
        stores.append(pltpu.make_async_copy(send_ref.at[here], send_out.at[here], sems.at[2 + chunks + g]))
        stores[-1].start()
    for store in stores:
        store.wait()


def fetch(role, own, near, far, here, sem):
    @pl.when(role == 0)
    def _():
        pltpu.make_async_copy(own, here, sem).start()

    @pl.when((role == 1) | (role == 2))
    def _():
        pltpu.make_async_copy(near, here, sem).start()

    @pl.when(role == 3)
    def _():
        pltpu.make_async_copy(far, here, sem).start()

    return pltpu.make_async_copy(near, here, sem)


def hidden_kernel(role_ref, in_hbm, own_gate, moved_gate, own_up, near_up, far_up, out_ref, in_ref, gate_ref, up_ref, sems):
    width = gate_ref.shape[0]
    sources = in_ref.shape[0]
    blocks, rows, _ = out_ref.shape
    both = rows // (GROUP * (MAIN + EXTRA))
    count = sources // blocks
    role = role_ref[0]
    loads = [
        pltpu.make_async_copy(in_hbm.at[pl.ds(b * count, count)], in_ref.at[pl.ds(b * count, count)], sems.at[2 + b])
        for b in range(blocks)
    ]
    loads[0].start()
    gate_load = fetch(role, own_gate, moved_gate, moved_gate, gate_ref, sems.at[0])
    up_load = fetch(role, own_up, near_up, far_up, up_ref, sems.at[1])
    for load in loads[1:]:
        load.start()
    for b in range(blocks):
        loads[b].wait()
        parts = []
        for j in range(both):
            here = pl.ds(b * count + j * GROUP, GROUP)
            parts.append(in_ref[here, :, 0:width].reshape(GROUP * MAIN, width))
        for j in range(both):
            here = pl.ds(b * count + j * GROUP, GROUP)
            parts.append(unfolded(in_ref[here, :, width:].reshape(PIECE, PIECE)))
        rows = jnp.concatenate(parts, 0)
        if b == 0:
            gate_load.wait()
        gate = dot(rows, gate_ref[...])
        if b == 0:
            up_load.wait()
        up = dot(rows, up_ref[...])
        out_ref[b] = (gate / (1.0 + jnp.exp(-gate)) * up).astype(jnp.bfloat16)


def left_kernel(role_ref, in_ref, own, near, far, out_ref, left_ref, sem):
    blocks, rows, _ = in_ref.shape
    both = rows // (GROUP * (MAIN + EXTRA))
    main = both * GROUP * MAIN
    start = out_ref.shape[2]
    fetch(role_ref[0], own.at[:, 0:start], near, far, left_ref, sem).wait()

    def block(b, carry):
        here = pl.ds(b * both * GROUP, both * GROUP)
        result = dot(in_ref[b, :main, :], left_ref[...]).astype(jnp.bfloat16)
        out_ref[here, :, :] = result.reshape(both * GROUP, MAIN, start)
        return carry

    lax.fori_loop(0, blocks, block, 0)


def right_kernel(
    role_ref, in_ref, own, near_left, far_left, near, far, out_ref, left_ref, right_ref, left_sem, right_sem
):
    start, width = left_ref.shape[1], right_ref.shape[1]
    blocks, rows, _ = in_ref.shape
    both = rows // (GROUP * (MAIN + EXTRA))
    main = both * GROUP * MAIN
    role = role_ref[0]
    right_load = fetch(role, own.at[:, start:], near, far, right_ref, right_sem)
    left_load = fetch(role, own.at[:, 0:start], near_left, far_left, left_ref, left_sem)
    right_load.wait()
    left_load.wait()

    def block(b, carry):
        here = pl.ds(b * both * GROUP, both * GROUP)
        result = dot(in_ref[b], right_ref[...]).astype(jnp.bfloat16)
        out_ref[here, :, 0:width] = result[:main].reshape(both * GROUP, MAIN, width)
        first = dot(in_ref[b, main:, :], left_ref[...]).astype(jnp.bfloat16)
        rest = jnp.concatenate([first, result[main:]], 1)
        for j in range(both):
            there = pl.ds((b * both + j) * GROUP, GROUP)
            piece = folded(rest[j * GROUP * EXTRA : (j + 1) * GROUP * EXTRA])
            out_ref[there, :, width:] = piece.reshape(GROUP, MAIN, PIECE)
        return carry

    lax.fori_loop(0, blocks, block, 0)


def weight_kernel(pair_ref, route_ref, score_ref, main_ref, extra_ref):
    tokens = route_ref.shape[0]
    experts = main_ref.shape[1] // MAIN
    expert = iota((tokens, experts), 1)
    first, second = route_ref[:, 0:1], route_ref[:, 1:2]
    is_first, is_second = expert == first, expert == second
    hits = (is_first | is_second).astype(jnp.bfloat16)
    earlier = (iota((tokens, tokens), 0) > iota((tokens, tokens), 1)).astype(jnp.bfloat16)
    counts = dot(earlier, hits)
    group = jax.nn.sigmoid(score_ref[:, 0:1])
    pair = score_ref[:, 1:2]
    weights = (group * jax.nn.sigmoid(pair), group * jax.nn.sigmoid(-pair))
    places = []
    for mask, named in ((is_first, first), (is_second, second)):
        rank = jnp.sum(jnp.where(mask, counts, 0.0), axis=1, keepdims=True).astype(jnp.int32)
        place = member_of(named, pair_ref[0])
        places.append(
            (
                jnp.where(rank < MAIN, place * MAIN + rank, -1),
                jnp.where((rank >= MAIN) & (rank < MAIN + EXTRA), place * EXTRA + rank - MAIN, -1),
            )
        )
    for ref, which in ((main_ref, 0), (extra_ref, 1)):
        n = ref.shape[1]
        step = min(n, 256)
        for low in range(0, n, step):
            column = iota((tokens, step), 1) + low
            value = jnp.where(column == places[0][which], weights[0], 0.0)
            value = jnp.where(column == places[1][which], weights[1], value)
            ref[:, low : low + step] = value.astype(jnp.bfloat16)


def combine_kernel(left_ref, right_ref, main_ref, extra_ref, out_ref, rest_ref):
    experts, _, start = left_ref.shape
    width = right_ref.shape[2] - PIECE
    for g in range(experts // GROUP):
        block = right_ref[g * GROUP : (g + 1) * GROUP, :, width:].reshape(PIECE, PIECE)
        rest_ref[g * 2 * GROUP : (g + 1) * 2 * GROUP, :] = unfolded(block)
    step = 256
    for ref, first, count in ((left_ref, 0, start), (right_ref, start, width)):

        def columns(i, carry):
            here = pl.ds(pl.multiple_of(i * step, step), step)
            there = pl.ds(pl.multiple_of(first + i * step, step), step)
            rows = ref[:, :, here].reshape(experts * MAIN, step)
            total = dot(main_ref[...], rows) + dot(extra_ref[...], rest_ref[:, there])
            out_ref[:, there] = total.astype(jnp.bfloat16)
            return carry

        lax.fori_loop(0, count // step, columns, 0)


VMEM = pl.BlockSpec(memory_space=pltpu.VMEM)
HBM = pl.BlockSpec(memory_space=pltpu.HBM)


def in_hbm(x):
    return pltpu.with_memory_space_constraint(x, pltpu.HBM)


SMEM = pl.BlockSpec(memory_space=pltpu.SMEM)


def call(kernel, outs, ins, out_specs, scratch, limit, flops, nbytes, *args):
    return pl.pallas_call(
        kernel,
        out_shape=outs,
        in_specs=ins,
        out_specs=out_specs,
        scratch_shapes=scratch,
        compiler_params=pltpu.CompilerParams(vmem_limit_bytes=limit << 20),
        cost_estimate=pl.CostEstimate(flops=flops, bytes_accessed=nbytes, transcendentals=0),
    )(*args)


def gated_rows(value, gate):
    return (value.astype(jnp.float32) * jax.nn.sigmoid(gate.astype(jnp.float32))).astype(
        jnp.bfloat16
    )


def conv_kernel(
    me_ref, b0, b1, b2, b3, taps_ref, gain_ref, shift_ref, own, m1, m2, m3, o1, o2, o3, out_ref, x_ref, f_ref
):
    halves, rows, lanes = f_ref.shape
    blocks = (b0, b1, b2, b3)
    peers = len(blocks)
    taps = taps_ref.shape[0]
    lead = b0.shape[0] - rows - (taps - 1)
    me, core = me_ref[0], me_ref[1]
    parts = [pl.ds(pl.multiple_of(h * lanes, lanes), lanes) for h in (core, 1 - core)]
    for k, block in enumerate(blocks):
        for h, part in enumerate(parts):
            x_ref[2 * k + h] = block[:, part].astype(jnp.float32)

    def columns(i):
        source = (me + peers - i // 2) % peers
        half = (core + i) % 2
        return pl.ds(pl.multiple_of((source * 2 + half) * lanes, lanes), lanes)

    step = 64

    def filtered(i, carry):
        cols = columns(i)
        total, squares = carry
        sums, sums2 = [], []
        for base in range(0, rows, step):
            value = taps_ref[0:1, cols] * x_ref[i, base + lead : base + lead + step, :]
            for j in range(1, taps):
                low = base + lead + j
                value = value + taps_ref[j : j + 1, cols] * x_ref[i, low : low + step, :]
            f_ref[i, base : base + step, :] = value
            sums.append(value)
            sums2.append(value * value)
        return total + jnp.concatenate(sums, 0), squares + jnp.concatenate(sums2, 0)

    zero = jnp.zeros((rows, lanes), jnp.float32)
    total, squares = lax.fori_loop(0, halves, filtered, (zero, zero))
    center = jnp.sum(total, axis=1, keepdims=True) / CONV
    spread = jnp.sum(squares, axis=1, keepdims=True) / CONV - center * center
    scale = lax.rsqrt(spread + 1e-05)
    acts = []
    for i in range(halves):
        cols = columns(i)
        normed = (f_ref[i] - center) * scale * gain_ref[:, cols] + shift_ref[:, cols]
        acts.append((normed / (1.0 + jnp.exp(-normed))).astype(jnp.bfloat16))
    acts = [jnp.concatenate(acts[2 * k : 2 * k + 2], 1) for k in range(peers)]
    width = 512
    for low in range(0, out_ref.shape[1], width):
        summed = jnp.zeros((rows, width), jnp.float32)
        cols = slice(low, low + width)
        pairs = [(own[parts[0], cols], own[parts[1], cols])]
        pairs += [(m[:, cols], o[:, cols]) for m, o in ((m1, o1), (m2, o2), (m3, o3))]
        for act, weight in zip(acts, pairs):
            partial = dot(act, jnp.concatenate(weight, 0)).astype(jnp.bfloat16)
            summed = summed + partial.astype(jnp.float32)
        out_ref[:, low : low + width] = summed.astype(jnp.bfloat16)


def conv_half(conv_value, conv_gate, depth_weight, norm_gain, norm_shift, conv_out_weight):
    length, channels = conv_value.shape
    peers = lax.axis_size("tp")
    me = lax.axis_index("tp").astype(jnp.int32)
    rows = length // peers
    reach = 32
    last = gated_rows(conv_value[length - reach :], conv_gate[length - reach :])
    earlier = lax.ppermute(last, AXES, HALO)
    padded = jnp.concatenate([earlier, gated_rows(conv_value, conv_gate)], 0)
    core = lax.axis_index("member").astype(jnp.int32) % 2
    half = channels // 2
    part = lax.dynamic_slice_in_dim(conv_out_weight, core * half, half, 0)
    blocks, mine, others = [], [], []
    for by in range(peers):
        peer = (me + by) % peers
        block = lax.dynamic_slice_in_dim(padded, peer * rows, rows + reach, 0)
        if by > 0:
            ring = [(i, (i + by) % peers) for i in range(peers)]
            block = lax.ppermute(block, "tp", ring)
            mine.append(lax.ppermute(part, "tp", ring))
            others.append(lax.ppermute(mine[-1], AXES, [(i, i ^ 4) for i in range(256)]))
        blocks.append(block)
    width = conv_out_weight.shape[1]

    def last(after):
        arrived, _ = lax.optimization_barrier((tuple(blocks), after))
        return project(arrived)

    def project(blocks):
        return call(
            conv_kernel,
            jax.ShapeDtypeStruct((rows, width), jnp.bfloat16),
            [SMEM] + [VMEM] * 14,
            VMEM,
            [
                pltpu.VMEM((2 * peers, rows + reach, channels // 2), jnp.float32),
                pltpu.VMEM((2 * peers, rows, channels // 2), jnp.float32),
            ],
            24,
            2 * rows * CONV * width,
            CONV * width * 2,
            jnp.stack([me, core]),
            *blocks,
            depth_weight,
            norm_gain[None, :],
            norm_shift[None, :],
            conv_out_weight,
            *mine,
            *others,
        )

    return last


def moe_half(moe_input, moe_gain, route_experts, route_scores, expert_gate, expert_up, expert_down, conv_last):
    tokens, width = moe_input.shape
    experts = 64
    hidden = expert_gate.shape[2]
    slots = experts * (MAIN + EXTRA)
    wide = jax.ShapeDtypeStruct((experts, MAIN, width + PIECE), jnp.bfloat16)
    pair = lax.axis_index("pair").astype(jnp.int32).reshape(1)
    role = hops_of(lax.axis_index("tp"), lax.axis_index("member") % 2).astype(jnp.int32).reshape(1)
    arrays = {
        "gates": expert_gate,
        "ups": expert_up,
        "lefts": expert_down[:, :, :LEFT],
        "rights": expert_down[:, :, LEFT:],
    }
    near, far = {}, {}
    for name, array in arrays.items():
        near[name] = lax.ppermute(array, AXES, weight_pairs("gate" if name == "gates" else "near"))
        if name != "gates":
            far[name] = lax.ppermute(near[name], AXES, weight_pairs("relay"))
    near = {name: in_hbm(array[0]) for name, array in near.items()}
    far = {name: in_hbm(array[0]) for name, array in far.items()}
    own_down = in_hbm(expert_down[0])
    send = call(
        send_kernel,
        pltpu.HBM(wide.shape, wide.dtype),
        [SMEM, HBM, HBM, HBM],
        HBM,
        [
            pltpu.VMEM((TOP, tokens), jnp.int32),
            pltpu.VMEM((tokens, width), jnp.bfloat16),
            pltpu.VMEM((1, width), jnp.float32),
            pltpu.VMEM((tokens, width), jnp.bfloat16),
            pltpu.VMEM((8, tokens), jnp.int32),
            pltpu.VMEM(wide.shape, jnp.bfloat16),
            pltpu.SemaphoreType.DMA((10,)),
        ],
        24,
        2 * slots * tokens * width,
        slots * width * 4,
        pair,
        in_hbm(route_experts.T),
        in_hbm(moe_input),
        in_hbm(moe_gain[None, :]),
    )
    arrived = lax.all_to_all(send, ("member", "tp"), split_axis=0, concat_axis=0, tiled=True)
    main, extra = call(
        weight_kernel,
        (
            jax.ShapeDtypeStruct((tokens, experts * MAIN), jnp.bfloat16),
            jax.ShapeDtypeStruct((tokens, experts * EXTRA), jnp.bfloat16),
        ),
        [SMEM, VMEM, VMEM],
        (VMEM, VMEM),
        [],
        16,
        2 * tokens * tokens * experts,
        4 * tokens * slots,
        pair,
        route_experts,
        route_scores,
    )
    weight = pltpu.VMEM((width, hidden), jnp.bfloat16)
    inner = call(
        hidden_kernel,
        jax.ShapeDtypeStruct((2, slots // 2, hidden), jnp.bfloat16),
        [SMEM] + [HBM] * 6,
        VMEM,
        [pltpu.VMEM(wide.shape, jnp.bfloat16), weight, weight, pltpu.SemaphoreType.DMA((4,))],
        32,
        4 * slots * width * hidden,
        slots * width * 2,
        role,
        in_hbm(arrived),
        in_hbm(expert_gate[0]),
        near["gates"],
        in_hbm(expert_up[0]),
        near["ups"],
        far["ups"],
    )
    first = call(
        left_kernel,
        jax.ShapeDtypeStruct((experts, MAIN, LEFT), jnp.bfloat16),
        [SMEM, VMEM] + [HBM] * 3,
        VMEM,
        [pltpu.VMEM((hidden, LEFT), jnp.bfloat16), pltpu.SemaphoreType.DMA],
        16,
        2 * slots * LEFT * hidden,
        slots * LEFT * 2,
        role,
        inner,
        own_down,
        near["lefts"],
        far["lefts"],
    )
    back1 = lax.all_to_all(first, ("member", "tp"), split_axis=0, concat_axis=0, tiled=True)
    conv_out = conv_last(inner)
    inner, conv_out, main, extra = lax.optimization_barrier((inner, conv_out, main, extra))
    second = call(
        right_kernel,
        jax.ShapeDtypeStruct((experts, MAIN, width - LEFT + PIECE), jnp.bfloat16),
        [SMEM, VMEM] + [HBM] * 5,
        VMEM,
        [
            pltpu.VMEM((hidden, LEFT), jnp.bfloat16),
            pltpu.VMEM((hidden, width - LEFT), jnp.bfloat16),
            pltpu.SemaphoreType.DMA,
            pltpu.SemaphoreType.DMA,
        ],
        16,
        2 * slots * (width - LEFT) * hidden,
        slots * width * 2,
        role,
        inner,
        own_down,
        near["lefts"],
        far["lefts"],
        near["rights"],
        far["rights"],
    )
    back2 = lax.all_to_all(second, ("member", "tp"), split_axis=0, concat_axis=0, tiled=True)
    moe_out = call(
        combine_kernel,
        jax.ShapeDtypeStruct((tokens, width), jnp.bfloat16),
        [VMEM] * 4,
        VMEM,
        [pltpu.VMEM((experts * EXTRA, width), jnp.bfloat16)],
        16,
        2 * slots * tokens * width,
        slots * width * 2,
        back1,
        back2,
        main,
        extra,
    )
    return conv_out, moe_out


def on_device(
    conv_value,
    conv_gate,
    depth_weight,
    norm_gain,
    norm_shift,
    conv_out_weight,
    moe_input,
    moe_gain,
    route_experts,
    route_scores,
    expert_gate,
    expert_up,
    expert_down,
):
    conv_last = conv_half(
        conv_value, conv_gate, depth_weight, norm_gain, norm_shift, conv_out_weight
    )
    return moe_half(
        moe_input,
        moe_gain,
        route_experts,
        route_scores,
        expert_gate,
        expert_up,
        expert_down,
        conv_last,
    )


def solution(mesh):
    ep = ("pair", "member")
    every = (*ep, "tp")
    mesh = jax.sharding.Mesh(mesh.devices.reshape(4, 16, 4), every)
    in_specs = (
        P(ep, "tp"),
        P(ep, "tp"),
        P(),
        P(),
        P(),
        P("tp", None),
        P(every, None),
        P(),
        P(every, None),
        P(every, None),
        P(ep, None, None),
        P(ep, None, None),
        P(ep, None, None),
    )
    out_specs = (P(every, None), P(every, None))
    return jax.shard_map(
        on_device, mesh=mesh, in_specs=in_specs, out_specs=out_specs, check_vma=False
    )
```
